512 devices in a mesh: sp: 64 (over z, y), fs: 4 (over x), tp: 2 (over core).
Axes of the slice: x: 4, y: 8, z: 8, core: 2. Of those that a mesh axis runs over, the one named last changes fastest.
Arguments:
- tokens: bfloat16 [32768, 2048], P(('fs', 'sp')), may hold values from -6 to 6
- in_gain: float32 [2048], replicated, may hold values from 0.1 to 1.9
- query_weight: bfloat16 [2048, 512], P(None, ('tp', 'fs')), may hold values from -0.17291713 to 0.17291713
- key_weight: bfloat16 [2048, 512], P(None, ('tp', 'fs')), may hold values from -0.17291713 to 0.17291713
- value_weight: bfloat16 [2048, 512], P(None, ('tp', 'fs')), may hold values from -0.125 to 0.125
- rec_query_weight: bfloat16 [2048, 512], P(None, ('tp', 'fs')), may hold values from -0.125 to 0.125
- rec_forget_weight: bfloat16 [2048, 512], P(None, ('tp', 'fs')), may hold values from -0.125 to 0.125
- rec_input_weight: bfloat16 [2048, 512], P(None, ('tp', 'fs')), may hold values from -0.125 to 0.125
- mix_lambda: float32 [4], P('tp'), may hold values from 0.3 to 0.8
- lower_bound: float32 [4, 128], P('tp'), may hold values from 0.9 to 0.9999695
- forget_scale: float32 [32768], P(('fs', 'sp')), may hold values from 0.35 to 24576
- att_gain: float32 [128], replicated, may hold values from 0.1 to 1.9
- recurrence_gain: float32 [128], replicated, may hold values from 0.1 to 1.9
- att_out_weight: bfloat16 [512, 2048], P('tp'), may hold values from -0.1875 to 0.1875
- rec_out_weight: bfloat16 [512, 2048], P('tp'), may hold values from -0.1875 to 0.1875
Outputs:
- mixed_out: bfloat16 [32768, 2048], P(('fs', 'sp'))
- log_weight_sum: float32 [4, 32768], P('tp', ('fs', 'sp'))
The draws below stay inside these ranges and needn't reach their ends.
All inputs are finite; a program needn't handle non-finite values.
Results may differ from the reference program's by a relative error of at most 0.012.
Values may be sent and summed in bfloat16 or wider, within the bound.
A program may use at most 128 MiB of HBM per device.

```python
import math
import jax
import jax.numpy as jnp
from jax import lax

D = 2048
HEADS = 4
DK = 64
DV = 128
BLK = 64
TOK_DEV = 128
LENGTH_PER_SEQ = 8192
SEQS = 4
TOKEN_COUNT_ALL = 32768
N_TP = 2


def drawn_weight(key, salt):
    spread = (D * 10 // 17) ** (-0.5)
    noise = jnp.clip(jax.random.normal(jax.random.fold_in(key, salt), (D, HEADS * 2 * DK), jnp.float32), -4.5, 4.5) * spread
    return jnp.clip(noise, -6.0 * spread, 6.0 * spread).astype(jnp.bfloat16)


def draw_tokens(key, part):
    base = jax.random.normal(jax.random.fold_in(key, 41), (TOKEN_COUNT_ALL, D), jnp.float32)
    return jnp.clip(base, -6.0, 6.0).astype(jnp.bfloat16)


def draw_query_weight(key, part):
    return drawn_weight(key, 51)


def draw_key_weight(key, part):
    return drawn_weight(key, 53)


def draw_lower_bound(key, part):
    first_key, second_key = jax.random.split(jax.random.fold_in(key, 11))
    slower = jax.random.uniform(first_key, (HEADS, DV), jnp.float32) < 0.5
    mixing = jax.random.uniform(second_key, (HEADS, DV), jnp.float32)
    slower_minimum = 0.25 / LENGTH_PER_SEQ
    slow_gap = jnp.exp(math.log(slower_minimum) + mixing * math.log(3.0))
    fast_gap = jnp.exp(math.log(0.04) + mixing * (math.log(0.1) - math.log(0.04)))
    return (1.0 - jnp.where(slower, slow_gap, fast_gap)).astype(jnp.float32)


def draw_forget_scale(key, part):
    key_collection = jax.random.split(jax.random.fold_in(key, 23), 4)
    device_factor = jnp.exp(math.log(0.5) + jax.random.uniform(key_collection[0], (TOKEN_COUNT_ALL // TOK_DEV,), jnp.float32) * math.log(4.0))
    block_factor = jnp.exp(jax.random.uniform(key_collection[1], (TOKEN_COUNT_ALL // BLK,), jnp.float32) * 0.6 - 0.3)
    initial_scale = jnp.repeat(device_factor, TOK_DEV) * jnp.repeat(block_factor, BLK)
    sudden_rows = jax.random.uniform(key_collection[2], (TOKEN_COUNT_ALL,), jnp.float32) < 2.5 / LENGTH_PER_SEQ
    height_per_level = LENGTH_PER_SEQ * (1.0 + 2.0 * jax.random.uniform(key_collection[3], (TOKEN_COUNT_ALL,), jnp.float32))
    return jnp.where(sudden_rows, height_per_level, initial_scale).astype(jnp.float32)


def shard_levels(rng, shape, cuts, least, largest):
    factor_of = 1.0
    for axis_at, shards_of in cuts:
        heights = jax.random.uniform(jax.random.fold_in(jax.random.fold_in(rng, 6), axis_at), (shards_of,), jnp.float32, least / len(cuts), largest / len(cuts))
        factor_of = factor_of * jnp.repeat(jnp.exp(heights), shape[axis_at] // shards_of).reshape((-1,) + (1,) * (len(shape) - 1 - axis_at))
    return factor_of


def bell_draw(rng, extent, scale, reach, cuts=(), kind=jnp.bfloat16):
    values = jax.random.normal(rng, extent, jnp.float32) * scale
    if len(cuts) > 0:
        values = shard_levels(rng, extent, cuts, -0.22, 0.18) * values
    return jnp.clip(values, min=-reach, max=reach).astype(kind)


def setup_inputs(seed: int = 0) -> dict:
    key_of = jax.random.split(jax.random.key(seed), 16)
    return {
        "tokens": draw_tokens(jax.random.fold_in(key_of[15], 71), 0),
        "in_gain": jnp.clip(1.0 + 0.18 * jax.random.normal(key_of[1], (D,), jnp.float32), 0.1, 1.9),
        "query_weight": draw_query_weight(jax.random.fold_in(key_of[15], 71), 0),
        "key_weight": draw_key_weight(jax.random.fold_in(key_of[15], 71), 0),
        "value_weight": bell_draw(key_of[4], (D, HEADS * DV), D ** -0.5, 0.125, ((1, 8),)),
        "rec_query_weight": bell_draw(key_of[5], (D, HEADS * DV), D ** -0.5, 0.125, ((1, 8),)),
        "rec_forget_weight": bell_draw(key_of[6], (D, HEADS * DV), D ** -0.5, 0.125, ((1, 8),)),
        "rec_input_weight": bell_draw(key_of[7], (D, HEADS * DV), D ** -0.5, 0.125, ((1, 8),)),
        "mix_lambda": jnp.clip(0.3 + 0.5 * jax.random.uniform(key_of[8], (HEADS,), jnp.float32) ** shard_levels(key_of[8], (HEADS,), ((0, 2),), -0.2, 0.2), 0.3, 0.8),
        "lower_bound": draw_lower_bound(jax.random.fold_in(key_of[15], 71), 0),
        "forget_scale": draw_forget_scale(jax.random.fold_in(key_of[15], 71), 0),
        "att_gain": jnp.clip(1.0 + 0.18 * jax.random.normal(key_of[11], (DV,), jnp.float32), 0.1, 1.9),
        "recurrence_gain": jnp.clip(1.0 + 0.18 * jax.random.normal(key_of[12], (DV,), jnp.float32), 0.1, 1.9),
        "att_out_weight": bell_draw(key_of[13], (HEADS * DV, D), (2 * HEADS * DV) ** -0.5, 0.1875, ((0, 2),)),
        "rec_out_weight": bell_draw(key_of[14], (HEADS * DV, D), (2 * HEADS * DV) ** -0.5, 0.1875, ((0, 2),)),
    }


EPS = 1e-06
NEG = -1e+30
QUERY_ROWS = 512

def norm_rows(values, gain):
    return values * lax.rsqrt(lax.optimization_barrier(jnp.mean(values * values, axis=-1, keepdims=True)) + EPS) * gain

def to_sequences(rows):
    return rows.reshape(SEQS, LENGTH_PER_SEQ, rows.shape[-1])

def from_sequences(seq_rows):
    return seq_rows.reshape(TOKEN_COUNT_ALL, seq_rows.shape[-1])

def block_recurrence(queries, key_in, value_in, log_forget):
    head_count, row_count, key_width = queries.shape
    block_count = row_count // BLK

    def to_blocks(array_in):
        return array_in.reshape(head_count, block_count, BLK, array_in.shape[-1]).transpose(1, 0, 2, 3)
    causal = jnp.tril(jnp.ones((BLK, BLK), bool))

    def advance(passed_state, inputs):
        query_block, key_block, value_block, l_blk = inputs
        accumulator_sum = jnp.cumsum(l_blk, axis=1)
        cross_block_output = jnp.einsum('sre,sei->sri', query_block * jnp.exp(accumulator_sum), passed_state, precision=lax.Precision.HIGHEST)
        spread = accumulator_sum[:, :, None, :] - accumulator_sum[:, None, :, :]
        decay = jnp.exp(jnp.where(causal[None, :, :, None], spread, -jnp.inf))
        scores = jnp.einsum('htk,htsk,hsk->hts', query_block, decay, key_block, precision=lax.Precision.HIGHEST)
        result = cross_block_output + jnp.einsum('hts,hsv->htv', scores, value_block, precision=lax.Precision.HIGHEST)
        final_log_sum = accumulator_sum[:, -1:, :]
        updated_state = jnp.exp(final_log_sum[:, 0, :])[:, :, None] * passed_state + jnp.einsum('plf,plt->pft', key_block * jnp.exp(final_log_sum - accumulator_sum), value_block, precision=lax.Precision.HIGHEST)
        return (updated_state, result)
    begin_state = jnp.zeros((head_count, key_width, value_in.shape[-1]), jnp.float32)
    end_state, results = lax.scan(advance, begin_state, (to_blocks(queries), to_blocks(key_in), to_blocks(value_in), to_blocks(log_forget)))
    return (end_state, results.transpose(1, 0, 2, 3).reshape(head_count, row_count, value_in.shape[-1]))

def attend_sequence(q_seq, k_seq, v_seq, mix_lambda, att_gain):
    length_now = q_seq.shape[0]
    queries = q_seq.reshape(length_now, HEADS, 2, DK).transpose(1, 2, 0, 3).astype(jnp.float32)
    key_heads = k_seq.reshape(length_now, HEADS, 2, DK).transpose(1, 2, 0, 3).astype(jnp.float32)
    head_values = v_seq.reshape(length_now, HEADS, DV).transpose(1, 0, 2).astype(jnp.float32)
    block_rows = min(QUERY_ROWS, length_now)
    key_pos = jnp.arange(length_now, dtype=jnp.int32)

    def one_block(block_index):
        begin_row = (block_index * block_rows).astype(jnp.int32)
        query_block = lax.dynamic_slice_in_dim(queries, begin_row, block_rows, 2)
        q_pos = begin_row + jnp.arange(block_rows, dtype=jnp.int32)
        allowed = q_pos[:, None] >= key_pos[None, :]
        scores = jnp.einsum('hmqd,hmkd->hmqk', query_block, key_heads) * DK ** (-0.5)
        scores = jnp.where(allowed, scores, NEG)
        highest = lax.optimization_barrier(jnp.max(scores, axis=-1))
        weights = jnp.exp(scores - highest[..., None])
        weight_sum = lax.optimization_barrier(jnp.sum(weights, axis=-1))
        rounded_weights = lax.optimization_barrier(weights.astype(jnp.bfloat16)).astype(jnp.float32)
        summed_values = jnp.einsum('itap,ipn->itan', rounded_weights, head_values)
        mixed = summed_values[:, 0] / weight_sum[:, 0, :, None] - mix_lambda[:, None, None] * summed_values[:, 1] / weight_sum[:, 1, :, None]
        result = (norm_rows(mixed, att_gain) * 0.8).astype(jnp.bfloat16)
        return (result.transpose(1, 0, 2).reshape(block_rows, HEADS * DV), highest[:, 0] + jnp.log(weight_sum[:, 0]))
    results, log_sums = lax.map(one_block, jnp.arange(length_now // block_rows, dtype=jnp.int32))
    return (results.reshape(length_now, HEADS * DV), log_sums.transpose(1, 0, 2).reshape(HEADS, length_now))

def recur_sequence(rq_seq, rf_seq, ri_seq, scale_seq, lower_bound, recurrence_gain):
    length_now = rq_seq.shape[0]

    def heads_first(array_in):
        return array_in.reshape(length_now, HEADS, DV).transpose(1, 0, 2).astype(jnp.float32)
    queries = heads_first(rq_seq)
    lower_edge = lower_bound[:, None, :]
    forget = lower_edge + (1.0 - lower_edge) * jax.nn.sigmoid(heads_first(rf_seq))
    log_forget = scale_seq[None, :, None] * jnp.log(forget)
    key_in = 1.0 - jnp.exp(log_forget)
    _, results = block_recurrence(queries, key_in, heads_first(ri_seq), log_forget)
    normed_out = norm_rows(results, recurrence_gain).astype(jnp.bfloat16)
    return normed_out.transpose(1, 0, 2).reshape(length_now, HEADS * DV)

def reference(tokens, in_gain, query_weight, key_weight, value_weight, rec_query_weight, rec_forget_weight, rec_input_weight, mix_lambda, lower_bound, forget_scale, att_gain, recurrence_gain, att_out_weight, rec_out_weight):
    normed = norm_rows(tokens.astype(jnp.float32), in_gain).astype(jnp.bfloat16)

    def project(weight):
        return to_sequences(jnp.dot(normed, weight, preferred_element_type=jnp.float32).astype(jnp.bfloat16))
    pieces = tuple((project(weight) for weight in (query_weight, key_weight, value_weight, rec_query_weight, rec_forget_weight, rec_input_weight)))
    scales = to_sequences(forget_scale[:, None])[:, :, 0]

    def per_sequence(inputs):
        q_seq, k_seq, v_seq, rq_seq, rf_seq, ri_seq, scale_seq = inputs
        att_rows, log_sums = attend_sequence(q_seq, k_seq, v_seq, mix_lambda, att_gain)
        rec_rows = recur_sequence(rq_seq, rf_seq, ri_seq, scale_seq, lower_bound, recurrence_gain)
        return (att_rows, rec_rows, log_sums)
    att_all, rec_all, log_all = lax.map(per_sequence, pieces + (scales,))
    att_all = from_sequences(att_all)
    rec_all = from_sequences(rec_all)
    log_weight_sum = from_sequences(log_all.transpose(0, 2, 1)).transpose(1, 0)
    group_width = HEADS * DV // N_TP
    mixed = jnp.zeros((TOKEN_COUNT_ALL, D), jnp.float32)
    for group in range(N_TP):
        lower_col = group * group_width
        upper_col = lower_col + group_width
        portion = jnp.dot(att_all[:, lower_col:upper_col], att_out_weight[lower_col:upper_col], preferred_element_type=jnp.float32)
        portion = portion + jnp.dot(rec_all[:, lower_col:upper_col], rec_out_weight[lower_col:upper_col], preferred_element_type=jnp.float32)
        mixed = mixed + lax.optimization_barrier(portion.astype(jnp.bfloat16)).astype(jnp.float32)
    return (mixed.astype(jnp.bfloat16), log_weight_sum)
```

```python
import functools

import jax
import jax.numpy as jnp
from jax import lax
from jax.experimental import pallas as pl
from jax.experimental.pallas import tpu as pltpu
from jax.sharding import PartitionSpec as P

DK = 64
DV = 128
ROWS = 128
COLS = 384
EPS = 1e-06
NEG = -1e30
FS = 4
PARTS = 4
MESH = pl.DeviceIdType.MESH
F32 = jnp.float32
BF16 = jnp.bfloat16


def dot_nn(a, b):
    return lax.dot_general(a, b, (((1,), (0,)), ((), ())), preferred_element_type=F32)


def dot_nt(a, b):
    return lax.dot_general(a, b, (((1,), (1,)), ((), ())), preferred_element_type=F32)


def norm_rows(values, gain):
    mean = jnp.mean(values * values, axis=-1, keepdims=True)
    return values * lax.rsqrt(mean + EPS) * gain


def kernel_body(
    nz, ny,
    tok_hbm, gain_ref, wq, wk, wv, wrq, wrf, wri, lam_ref, lb_ref, scale_ref, attg_ref, recg_ref,
    wa_hbm, wr_hbm,
    out_ref, lws_ref,
    tok, wraw, wcat, wo, nrm, res, rsend,
    gy, gz, s_scr, e_scr,
    o0s, o0r, t0s, t0r, o1s, o1r, t1s, t1r,
    st_s, st_r, tot_s, tot_r, in_s, in_r, pref, qc_scr, ol_scr,
    pbuf, prx,
    lsem, a_send, a_recv, r_send, r_recv,
    gy_send, gy_recv, gz_send, gz_recv,
    o0_send, o0_recv, t0_send, t0_recv, o1_send, o1_recv, t1_send, t1_recv,
    st_send, st_recv, tot_send, tot_recv, in_send, in_recv,
    p_send, p_recv,
):
    p = lax.axis_index("sp")
    x = lax.axis_index("fs")
    t = lax.axis_index("tp")
    z = p // ny
    y = p % ny
    t_other = 1 - t
    xl = (x + 3) % 4
    xr = (x + 1) % 4
    xo = (x + 2) % 4
    slice_rows = DV // ny

    weights = (wq, wk, wv, wrq, wrf, wri)
    tok_copy = pltpu.make_async_copy(tok_hbm, tok, lsem.at[0])
    tok_copy.start()
    w_copies = [pltpu.make_async_copy(w, wraw.at[i], lsem.at[1 + i]) for i, w in enumerate(weights)]
    for c in w_copies:
        c.start()
    wo_copies = [
        pltpu.make_async_copy(wa_hbm, wo.at[0], lsem.at[7]),
        pltpu.make_async_copy(wr_hbm, wo.at[1], lsem.at[8]),
    ]
    for c in wo_copies:
        c.start()

    barrier = pltpu.get_barrier_semaphore()

    def greet(dev):
        pl.semaphore_signal(barrier, inc=1, device_id=dev, device_id_type=MESH)

    greet({"tp": t_other})
    for d in range(1, 4):
        greet({"fs": (x + d) % 4})
    for d in range(1, ny):
        greet({"sp": z * ny + (y + d) % ny})
    for d in range(1, nz):
        greet({"sp": ((z + d) % nz) * ny + y})

    def remote(src, dst, ssem, rsem, dev):
        return pltpu.make_async_remote_copy(
            src_ref=src, dst_ref=dst, send_sem=ssem, recv_sem=rsem, device_id=dev, device_id_type=MESH
        )

    def piece(f, tt, pc):
        return nrm.at[f, pl.ds(pl.multiple_of(tt * 64 + pc * 32, 32), 32)]

    def a_sem(f, tt, pc):
        return a_recv.at[f, tt * 2 + pc]

    def normalise(tt, pc):
        rows = pl.ds(pl.multiple_of(tt * 64 + pc * 32, 32), 32)
        nrm[x, rows, :] = norm_rows(tok[rows, :].astype(F32), gain_ref[...]).astype(BF16)

    tok_copy.wait()
    normalise(t, 0)
    normalise(t, 1)
    pl.semaphore_wait(barrier, 1 + 3 + (ny - 1) + (nz - 1))

    a_list = []

    def a_start(k, f, pc, dev):
        c = remote(piece(f, t, pc), piece(f, t, pc), a_send.at[k], a_sem(f, t, pc), dev)
        c.start()
        a_list.append(c)

    def a_wait(f, tt, pc):
        remote(piece(f, tt, pc), piece(f, tt, pc), a_send.at[0], a_sem(f, tt, pc), {"fs": xr}).wait_recv()

    a_start(0, x, 0, {"fs": xr})
    a_start(1, x, 1, {"fs": xl})
    a_start(2, x, 1, {"fs": xr})
    a_start(3, x, 0, {"fs": xl})
    normalise(t_other, 0)
    normalise(t_other, 1)
    for i in range(6):
        w_copies[i].wait()
        wcat[:, i * 64:(i + 1) * 64] = wraw[i]

    def project(f):
        return dot_nn(nrm[f], wcat[...]).astype(BF16)

    res[x] = project(x)
    a_wait(xl, t, 0)
    a_start(4, xl, 0, {"fs": xr})
    a_start(5, xl, 0, {"tp": t_other})
    a_wait(xr, t, 1)
    a_start(6, xr, 1, {"fs": xl})
    a_start(7, xr, 1, {"tp": t_other})
    a_wait(xl, t, 1)
    a_start(8, xl, 1, {"tp": t_other})
    a_wait(xr, t, 0)
    a_start(9, xr, 0, {"tp": t_other})

    r_list = []

    def answer(k, f):
        a_wait(f, t_other, 0)
        a_wait(f, t_other, 1)
        rsend[k] = project(f)
        c = remote(rsend.at[k], res.at[x], r_send.at[k], r_recv.at[x], {"fs": f})
        c.start()
        r_list.append(c)

    answer(0, xl)
    answer(1, xr)
    a_wait(xo, t, 0)
    a_start(10, xo, 0, {"tp": t_other})
    a_wait(xo, t, 1)
    a_start(11, xo, 1, {"tp": t_other})
    answer(2, xo)
    for f in (xl, xr, xo):
        remote(res.at[f], res.at[f], r_send.at[0], r_recv.at[f], {"fs": xr}).wait_recv()

    def tile(kind, h):
        lo = kind * 64
        return jnp.concatenate([res[2 * h, :, lo:lo + 64], res[2 * h + 1, :, lo:lo + 64]], axis=1)

    def value_t(h):
        return tile(2, h).astype(F32).T.astype(BF16)

    scale_q = jnp.asarray(DK ** (-0.5), BF16)
    gy[y, 0] = tile(0, 0) * scale_q
    gy[y, 1] = tile(1, 1)
    gy[y, 2] = value_t(1)
    gz[z, 0] = tile(0, 1) * scale_q
    gz[z, 1] = tile(1, 0)
    gz[z, 2] = value_t(0)

    def y_dev(yy):
        return {"sp": z * ny + yy}

    def z_dev(zz):
        return {"sp": zz * ny + y}

    g_list = []
    for d in range(1, max(ny, nz)):
        if d < ny:
            c = remote(gy.at[y], gy.at[y], gy_send.at[d], gy_recv.at[y], y_dev((y + d) % ny))
            c.start()
            g_list.append(c)
        if d < nz:
            c = remote(gz.at[z], gz.at[z], gz_send.at[d], gz_recv.at[z], z_dev((z + d) % nz))
            c.start()
            g_list.append(c)

    row = lax.broadcasted_iota(jnp.int32, (ROWS, ROWS), 0)
    col = lax.broadcasted_iota(jnp.int32, (ROWS, ROWS), 1)
    tril = jnp.where(row >= col, 1.0, 0.0).astype(F32)
    scale_col = jnp.broadcast_to(scale_ref[...], (ROWS, ROWS)).T
    for h in range(2):
        rq = tile(3, h).astype(F32)
        rf = tile(4, h).astype(F32)
        ri = tile(5, h)
        edge = lb_ref[h:h + 1, :]
        forget = edge + (1.0 - edge) * jax.nn.sigmoid(rf)
        g = scale_col * jnp.log(forget)
        kk = 1.0 - jnp.exp(g)
        cum = lax.dot_general(
            tril, g, (((1,), (0,)), ((), ())), precision=lax.Precision.HIGHEST, preferred_element_type=F32
        )
        scores = jnp.where(row == col, jnp.sum(rq * kk, axis=-1, keepdims=True), 0.0)
        c8 = cum.reshape(ROWS // 8, 8, DV)
        r8 = lax.broadcasted_iota(jnp.int32, (ROWS // 8, 8, DV), 1)
        for b in (64, 32, 16, 8, 4, 2, 1):
            if b >= 8:
                c3 = cum.reshape(ROWS // (2 * b), 2 * b, DV)
                diff = (c3 - c3[:, b - 1:b, :]).reshape(ROWS, DV)
            else:
                mid = c8[:, b - 1:b, :]
                for first in range(2 * b, 8, 2 * b):
                    mid = jnp.where(r8 >= first, c8[:, first + b - 1:first + b, :], mid)
                diff = (c8 - mid).reshape(ROWS, DV)
            upper = (row & (2 * b - 1)) >= b
            decay = jnp.exp(jnp.where(upper, diff, -diff))
            late = jnp.where(upper, rq * decay, 0.0).astype(BF16)
            early = jnp.where(upper, 0.0, kk * decay).astype(BF16)
            level = dot_nt(late, early)
            scores = scores + jnp.where((row ^ col) < 2 * b, level, 0.0)
        ol_scr[h] = dot_nn(scores.astype(BF16), ri)
        last = cum[ROWS - 1:ROWS, :]
        key_end = (kk * jnp.exp(last - cum)).astype(BF16)
        state_t = dot_nn(ri.astype(F32).T.astype(BF16), key_end)
        qc_scr[h] = (rq * jnp.exp(cum)).astype(BF16)
        st_s[:, h * slice_rows:(h + 1) * slice_rows, :] = state_t.reshape(ny, slice_rows, DV)
        st_s[:, 2 * slice_rows + 8 * h:2 * slice_rows + 8 * h + 8, :] = jnp.broadcast_to(
            jnp.exp(last).reshape(1, 1, DV), (ny, 8, DV)
        )
    st_r[y] = st_s[y]
    for d in range(1, ny):
        yy = (y + d) % ny
        c = remote(st_s.at[yy], st_r.at[y], st_send.at[d], st_recv.at[y], y_dev(yy))
        c.start()
        g_list.append(c)

    for d in range(1, ny):
        yy = (y + d) % ny
        remote(st_r.at[yy], st_r.at[yy], st_send.at[0], st_recv.at[yy], y_dev(yy)).wait_recv()
    half = slice_rows
    for h in range(2):
        state = jnp.zeros((half, DV), F32)
        rate = jnp.ones((8, DV), F32)
        for k in range(ny):
            pref[k, h * half:(h + 1) * half, :] = state
            pref[k, 2 * half + 8 * h:2 * half + 8 * h + 8, :] = rate
            step = st_r[k, 2 * half + 8 * h:2 * half + 8 * h + 8, :]
            state = step[0:1, :] * state + st_r[k, h * half:(h + 1) * half, :]
            rate = rate * step
        tot_s[h * half:(h + 1) * half, :] = state
        tot_s[2 * half + 8 * h:2 * half + 8 * h + 8, :] = rate
    for d in range(1, nz):
        zz = (z + d) % nz
        c = remote(tot_s, tot_r.at[z], tot_send.at[d], tot_recv.at[z], z_dev(zz))
        c.start()
        g_list.append(c)

    for d in range(1, nz):
        zz = (z + d) % nz
        remote(tot_r.at[zz], tot_r.at[zz], tot_send.at[0], tot_recv.at[zz], z_dev(zz)).wait_recv()

    def fold(k, carry):
        s0, s1 = carry
        d0 = tot_r[k, 2 * half:2 * half + 1, :]
        d1 = tot_r[k, 2 * half + 8:2 * half + 9, :]
        return (d0 * s0 + tot_r[k, 0:half, :], d1 * s1 + tot_r[k, half:2 * half, :])

    entry = lax.fori_loop(0, z, fold, (jnp.zeros((half, DV), F32), jnp.zeros((half, DV), F32)))
    for k in range(ny):
        for h in range(2):
            d = pref[k, 2 * half + 8 * h:2 * half + 8 * h + 1, :]
            in_s[k, h] = (d * entry[h] + pref[k, h * half:(h + 1) * half, :]).astype(BF16)
    in_r[y] = in_s[y]
    for d in range(1, ny):
        yy = (y + d) % ny
        c = remote(in_s.at[yy], in_r.at[y], in_send.at[d], in_recv.at[y], y_dev(yy))
        c.start()
        g_list.append(c)

    for d in range(1, ny):
        yy = (y + d) % ny
        remote(gy.at[yy], gy.at[yy], gy_send.at[0], gy_recv.at[yy], y_dev(yy)).wait_recv()
    for d in range(1, nz):
        zz = (z + d) % nz
        remote(gz.at[zz], gz.at[zz], gz_send.at[0], gz_recv.at[zz], z_dev(zz)).wait_recv()

    lane = lax.broadcasted_iota(jnp.int32, (ROWS, DV), 1)

    def unit(queries, tiles, count, limits, masked_from, o_out, t_out):
        zero = jnp.zeros_like(queries)
        both = jnp.concatenate(
            [jnp.where(lane < DK, queries, zero), jnp.where(lane < DK, zero, queries)], axis=0
        )
        top = jnp.full((8, 2 * ROWS), NEG, F32)
        for k in range(count):
            s = dot_nt(tiles[k, 1], both)
            if k >= masked_from:
                ri_ = lax.broadcasted_iota(jnp.int32, (ROWS, 2 * ROWS), 0)
                ci_ = lax.broadcasted_iota(jnp.int32, (ROWS, 2 * ROWS), 1) & (ROWS - 1)
                s = jnp.where(ri_ - ci_ <= limits(k), s, NEG)
            s_scr[k] = s
            top = jnp.maximum(top, jnp.max(s.reshape(ROWS // 8, 8, 2 * ROWS), axis=0))
        top = jnp.max(top, axis=0, keepdims=True)
        total = jnp.zeros((8, 2 * ROWS), F32)
        num = jnp.zeros((DV, 2 * ROWS), F32)
        for k in range(count):
            e = jnp.exp(s_scr[k] - top)
            total = total + jnp.sum(e.reshape(ROWS // 8, 8, 2 * ROWS), axis=0)
            num = num + dot_nn(tiles[k, 2], e.astype(BF16))
        total = jnp.sum(total, axis=0, keepdims=True)
        o_out[...] = num.astype(BF16)
        t_out[0:1, :] = top
        t_out[1:2, :] = total

    def head0(count):
        def body(yq, carry):
            unit(
                gy[yq, 0], gz, count,
                lambda k: ((z - k) * ny + (yq - y)) * ROWS,
                count - 2, o0s.at[yq], t0s.at[yq],
            )

            @pl.when(yq != y)
            def _():
                remote(o0s.at[yq], o0r.at[y], o0_send.at[yq], o0_recv.at[y], y_dev(yq)).start()
                remote(t0s.at[yq], t0r.at[y], t0_send.at[yq], t0_recv.at[y], y_dev(yq)).start()

            return carry

        lax.fori_loop(0, ny, body, 0)

    for count in range(2, nz + 1, 2):
        pl.when(z // 2 == count // 2 - 1)(functools.partial(head0, count))
    o0r[y] = o0s[y]
    t0r[y] = t0s[y]

    def head1(zq, carry):
        unit(gz[zq, 0], gy, ny, lambda k: 0, ny, o1s.at[zq], t1s.at[zq])
        remote(o1s.at[zq], o1r.at[z], o1_send.at[zq], o1_recv.at[z], z_dev(zq)).start()
        remote(t1s.at[zq], t1r.at[z], t1_send.at[zq], t1_recv.at[z], z_dev(zq)).start()
        return carry

    lax.fori_loop(z + 1, nz, head1, 0)
    unit(gz[z, 0], gy, ny, lambda k: (y - k) * ROWS, 0, o1r.at[z], t1r.at[z])

    for d in range(1, ny):
        yy = (y + d) % ny
        remote(in_r.at[yy], in_r.at[yy], in_send.at[0], in_recv.at[yy], y_dev(yy)).wait_recv()
    rec = []
    for h in range(2):
        o = ol_scr[h] + dot_nt(qc_scr[h], in_r[:, h].reshape(DV, DV))
        rec.append(norm_rows(o, recg_ref[...]).astype(BF16))
    rec_rows = jnp.concatenate(rec, axis=1)

    def merge(o_ref, t_ref, k, carry):
        top, total, num = carry
        t_new = t_ref[k]
        now = jnp.maximum(top, t_new[0:1, :])
        old_w = jnp.exp(top - now)
        new_w = jnp.exp(t_new[0:1, :] - now)
        total = old_w * total + new_w * t_new[1:2, :]
        num = old_w * num + new_w * o_ref[k].astype(F32)
        return (now, total, num)

    start = (
        jnp.full((1, 2 * ROWS), NEG, F32), jnp.zeros((1, 2 * ROWS), F32), jnp.zeros((DV, 2 * ROWS), F32)
    )

    def finish(h, carry):
        top, total, num = carry
        att = num[:, :ROWS] / total[:, :ROWS] - lam_ref[h] * num[:, ROWS:] / total[:, ROWS:]
        att = att * lax.rsqrt(jnp.mean(att * att, axis=0, keepdims=True) + EPS)
        lws_ref[h:h + 1, :] = top[:, :ROWS] + jnp.log(total[:, :ROWS])
        return (att.T * attg_ref[...] * 0.8).astype(BF16)

    def merge0(k, carry):
        @pl.when(k != y)
        def _():
            remote(o0r.at[k], o0r.at[k], o0_send.at[0], o0_recv.at[k], y_dev(y)).wait_recv()
            remote(t0r.at[k], t0r.at[k], t0_send.at[0], t0_recv.at[k], y_dev(y)).wait_recv()

        return merge(o0r, t0r, k, carry)

    def merge1(k, carry):
        @pl.when(k != z)
        def _():
            remote(o1r.at[k], o1r.at[k], o1_send.at[0], o1_recv.at[k], z_dev(z)).wait_recv()
            remote(t1r.at[k], t1r.at[k], t1_send.at[0], t1_recv.at[k], z_dev(z)).wait_recv()

        return merge(o1r, t1r, k, carry)

    att0 = finish(0, lax.fori_loop(0, ny, merge0, start))
    att1 = finish(1, lax.fori_loop(0, z + 1, merge1, start))
    att_rows = jnp.concatenate([att0, att1], axis=1)

    for c in wo_copies:
        c.wait()
    width = wo.shape[2] // PARTS
    p_list = []
    for k in range(PARTS):
        cols = slice(k * width, (k + 1) * width)
        part = dot_nn(att_rows, wo[0, :, cols]) + dot_nn(rec_rows, wo[1, :, cols])
        pbuf[k] = part.astype(BF16)
        c = remote(pbuf.at[k], prx.at[k], p_send.at[k], p_recv.at[k], {"tp": t_other})
        c.start()
        p_list.append(c)
    for k in range(PARTS):
        p_list[k].wait_recv()
        out_ref[:, k * width:(k + 1) * width] = (pbuf[k].astype(F32) + prx[k].astype(F32)).astype(BF16)

    for c in a_list + r_list + g_list + p_list:
        c.wait_send()

    def sent0(k, carry):
        @pl.when(k != y)
        def _():
            remote(o0s.at[k], o0r.at[y], o0_send.at[k], o0_recv.at[y], y_dev(k)).wait_send()
            remote(t0s.at[k], t0r.at[y], t0_send.at[k], t0_recv.at[y], y_dev(k)).wait_send()

        return carry

    lax.fori_loop(0, ny, sent0, 0)

    def sent1(k, carry):
        remote(o1s.at[k], o1r.at[z], o1_send.at[k], o1_recv.at[z], z_dev(k)).wait_send()
        remote(t1s.at[k], t1r.at[z], t1_send.at[k], t1_recv.at[z], z_dev(k)).wait_send()
        return carry

    lax.fori_loop(z + 1, nz, sent1, 0)


def on_device(nz, ny, tokens, in_gain, wq, wk, wv, wrq, wrf, wri, lam, lb, scale, attg, recg, wa, wr):
    d = tokens.shape[1]
    out_cols = wa.shape[1]
    any_spec = pl.BlockSpec(memory_space=pl.ANY)
    vmem = pl.BlockSpec(memory_space=pltpu.VMEM)
    smem = pl.BlockSpec(memory_space=pltpu.SMEM)
    slice_rows = DV // ny
    st_rows = 2 * slice_rows + 16
    dma = pltpu.SemaphoreType.DMA
    scratch = [
        pltpu.VMEM((ROWS, d), BF16),
        pltpu.VMEM((6, d, DK), BF16),
        pltpu.VMEM((d, COLS), BF16),
        pltpu.VMEM((2, wa.shape[0], out_cols), BF16),
        pltpu.VMEM((FS, ROWS, d), BF16),
        pltpu.VMEM((FS, ROWS, COLS), BF16),
        pltpu.VMEM((3, ROWS, COLS), BF16),
        pltpu.VMEM((ny, 3, ROWS, DV), BF16),
        pltpu.VMEM((nz, 3, ROWS, DV), BF16),
        pltpu.VMEM((max(ny, nz), ROWS, 2 * ROWS), F32),
        pltpu.VMEM((8, 128), F32),
        pltpu.VMEM((ny, DV, 2 * ROWS), BF16),
        pltpu.VMEM((ny, DV, 2 * ROWS), BF16),
        pltpu.VMEM((ny, 8, 2 * ROWS), F32),
        pltpu.VMEM((ny, 8, 2 * ROWS), F32),
        pltpu.VMEM((nz, DV, 2 * ROWS), BF16),
        pltpu.VMEM((nz, DV, 2 * ROWS), BF16),
        pltpu.VMEM((nz, 8, 2 * ROWS), F32),
        pltpu.VMEM((nz, 8, 2 * ROWS), F32),
        pltpu.VMEM((ny, st_rows, DV), F32),
        pltpu.VMEM((ny, st_rows, DV), F32),
        pltpu.VMEM((st_rows, DV), F32),
        pltpu.VMEM((nz, st_rows, DV), F32),
        pltpu.VMEM((ny, 2, slice_rows, DV), BF16),
        pltpu.VMEM((ny, 2, slice_rows, DV), BF16),
        pltpu.VMEM((ny, st_rows, DV), F32),
        pltpu.VMEM((2, ROWS, DV), BF16),
        pltpu.VMEM((2, ROWS, DV), F32),
        pltpu.VMEM((PARTS, ROWS, out_cols // PARTS), BF16),
        pltpu.VMEM((PARTS, ROWS, out_cols // PARTS), BF16),
        dma((9,)), dma((12,)), dma((FS, 4)), dma((3,)), dma((FS,)),
        dma((ny,)), dma((ny,)), dma((nz,)), dma((nz,)),
        dma((ny,)), dma((ny,)), dma((ny,)), dma((ny,)),
        dma((nz,)), dma((nz,)), dma((nz,)), dma((nz,)),
        dma((ny,)), dma((ny,)), dma((nz,)), dma((nz,)), dma((ny,)), dma((ny,)),
        dma((PARTS,)), dma((PARTS,)),
    ]
    return pl.pallas_call(
        functools.partial(kernel_body, nz, ny),
        out_shape=(
            jax.ShapeDtypeStruct((ROWS, out_cols), BF16),
            jax.ShapeDtypeStruct((2, ROWS), F32),
        ),
        in_specs=[any_spec, vmem] + [any_spec] * 6 + [smem, vmem, vmem, vmem, vmem, any_spec, any_spec],
        out_specs=(vmem, vmem),
        scratch_shapes=scratch,
        compiler_params=pltpu.CompilerParams(
            collective_id=0, has_side_effects=True, vmem_limit_bytes=56 * 1024 * 1024
        ),
    )(
        tokens, in_gain.reshape(1, d), wq, wk, wv, wrq, wrf, wri, lam, lb,
        scale.reshape(1, ROWS), attg.reshape(1, DV), recg.reshape(1, DV), wa, wr,
    )


def solution(mesh):
    sp = mesh.shape["sp"]
    nz = 1
    while nz * nz < sp:
        nz *= 2
    ny = sp // nz
    col_split = P(None, ("tp", "fs"))
    placed = (
        P(("fs", "sp"), None), P(),
        col_split, col_split, col_split, col_split, col_split, col_split,
        P("tp"), P("tp", None), P(("fs", "sp")), P(), P(),
        P("tp", None), P("tp", None),
    )
    return jax.shard_map(
        functools.partial(on_device, nz, ny),
        mesh=mesh,
        in_specs=placed,
        out_specs=(P(("fs", "sp"), None), P("tp", ("fs", "sp"))),
        check_vma=False,
    )
```

```python
import functools

import jax
import jax.numpy as jnp
from jax import lax
from jax.experimental import pallas as pl
from jax.experimental.pallas import tpu as pltpu
from jax.sharding import PartitionSpec as P

DK = 64
DV = 128
ROWS = 128
COLS = 384
EPS = 1e-06
NEG = -1e30
FS = 4
PARTS = 4
MESH = pl.DeviceIdType.MESH
F32 = jnp.float32
BF16 = jnp.bfloat16


def dot_nn(a, b):
    return lax.dot_general(a, b, (((1,), (0,)), ((), ())), preferred_element_type=F32)


def dot_nt(a, b):
    return lax.dot_general(a, b, (((1,), (1,)), ((), ())), preferred_element_type=F32)


def pack_rates(first, second):
    parts = []
    for rate in (first, second):
        high = rate.astype(BF16).astype(F32)
        parts += [jnp.broadcast_to(v, (4, DV)) for v in (high, rate - high)]
    return jnp.concatenate(parts, axis=0).astype(BF16)


def unpack_rates(packed):
    wide = packed.astype(F32)
    return wide[0:1] + wide[4:5], wide[8:9] + wide[12:13]


def norm_rows(values, gain):
    mean = jnp.mean(values * values, axis=-1, keepdims=True)
    return values * lax.rsqrt(mean + EPS) * gain


def kernel_body(
    nz, ny,
    tok_hbm, gain_ref, wq, wk, wv, wrq, wrf, wri, lam_ref, lb_ref, scale_ref, attg_ref, recg_ref,
    wa_hbm, wr_hbm,
    out_ref, lws_ref,
    tok, wcat, wo, nrm, res, rsend,
    gy, gz, s_scr, e_scr, vt,
    o0s, o0r, t0s, t0r, o1s, o1r, t1s, t1r,
    st_s, st_r, tot_s, tot_r, in_s, in_r, pref, qc_scr, ol_scr,
    pbuf, prx,
    lsem, a_send, a_recv, r_send, r_recv,
    gy_send, gy_recv, gz_send, gz_recv,
    o0_send, o0_recv, t0_send, t0_recv, o1_send, o1_recv, t1_send, t1_recv,
    st_send, st_recv, tot_send, tot_recv, in_send, in_recv,
    p_send, p_recv,
):
    p = lax.axis_index("sp")
    x = lax.axis_index("fs")
    t = lax.axis_index("tp")
    z = p // ny
    y = p % ny
    t_other = 1 - t
    xl = (x + 3) % 4
    xr = (x + 1) % 4
    xo = (x + 2) % 4
    slice_rows = DV // ny

    open_scope = []

    def phase(name):
        if open_scope:
            open_scope.pop().__exit__(None, None, None)
        if name:
            scope = jax.named_scope(name)
            scope.__enter__()
            open_scope.append(scope)

    phase("start")
    weights = (wq, wk, wv, wrq, wrf, wri)
    tok_copy = pltpu.make_async_copy(tok_hbm, tok, lsem.at[0])
    tok_copy.start()
    w_copies = [
        pltpu.make_async_copy(w, wcat.at[pl.ds(i * DK, DK)], lsem.at[1 + i]) for i, w in enumerate(weights)
    ]
    for c in w_copies:
        c.start()
    wo_copies = [
        pltpu.make_async_copy(wa_hbm, wo.at[0], lsem.at[7]),
        pltpu.make_async_copy(wr_hbm, wo.at[1], lsem.at[8]),
    ]
    for c in wo_copies:
        c.start()

    barrier = pltpu.get_barrier_semaphore()

    def greet(dev):
        pl.semaphore_signal(barrier, inc=1, device_id=dev, device_id_type=MESH)

    greet({"tp": t_other})
    for d in range(1, 4):
        greet({"fs": (x + d) % 4})
    for d in range(1, ny):
        greet({"sp": z * ny + (y + d) % ny})
    for d in range(1, nz):
        greet({"sp": ((z + d) % nz) * ny + y})

    def remote(src, dst, ssem, rsem, dev):
        return pltpu.make_async_remote_copy(
            src_ref=src, dst_ref=dst, send_sem=ssem, recv_sem=rsem, device_id=dev, device_id_type=MESH
        )

    def piece(f, tt, pc):
        return nrm.at[f, pl.ds(pl.multiple_of(tt * 64 + pc * 32, 32), 32)]

    def a_sem(f, tt, pc):
        return a_recv.at[f, tt * 2 + pc]

    def normalise(tt, pc):
        rows = pl.ds(pl.multiple_of(tt * 64 + pc * 32, 32), 32)
        nrm[x, rows, :] = norm_rows(tok[rows, :].astype(F32), gain_ref[...]).astype(BF16)

    tok_copy.wait()
    normalise(t, 0)
    normalise(t, 1)
    phase("entry_barrier")
    pl.semaphore_wait(barrier, 1 + 3 + (ny - 1) + (nz - 1))

    a_list = []

    def a_start(k, f, pc, dev):
        c = remote(piece(f, t, pc), piece(f, t, pc), a_send.at[k], a_sem(f, t, pc), dev)
        c.start()
        a_list.append(c)

    def a_wait(f, tt, pc):
        remote(piece(f, tt, pc), piece(f, tt, pc), a_send.at[0], a_sem(f, tt, pc), {"fs": xr}).wait_recv()

    phase("x_own")
    a_start(0, x, 0, {"fs": xr})
    a_start(1, x, 1, {"fs": xl})
    a_start(2, x, 1, {"fs": xr})
    a_start(3, x, 0, {"fs": xl})
    normalise(t_other, 0)
    normalise(t_other, 1)
    for i in range(6):
        w_copies[i].wait()

    def project(f):
        return dot_nt(nrm[f], wcat[...]).astype(BF16)

    res[x] = project(x)
    phase("x_forward")
    a_wait(xl, t, 0)
    a_start(4, xl, 0, {"fs": xr})
    a_start(5, xl, 0, {"tp": t_other})
    a_wait(xr, t, 1)
    a_start(6, xr, 1, {"fs": xl})
    a_start(7, xr, 1, {"tp": t_other})
    a_wait(xl, t, 1)
    a_start(8, xl, 1, {"tp": t_other})
    a_wait(xr, t, 0)
    a_start(9, xr, 0, {"tp": t_other})

    r_list = []

    def answer(k, f):
        a_wait(f, t_other, 0)
        a_wait(f, t_other, 1)
        rsend[k] = project(f)
        c = remote(rsend.at[k], res.at[x], r_send.at[k], r_recv.at[x], {"fs": f})
        c.start()
        r_list.append(c)

    phase("x_near")
    answer(0, xl)
    answer(1, xr)
    phase("x_far")
    a_wait(xo, t, 0)
    a_start(10, xo, 0, {"tp": t_other})
    a_wait(xo, t, 1)
    a_start(11, xo, 1, {"tp": t_other})
    answer(2, xo)
    phase("x_answers")
    for f in (xl, xr, xo):
        remote(res.at[f], res.at[f], r_send.at[0], r_recv.at[f], {"fs": xr}).wait_recv()

    phase("tiles")
    def tile(kind, h):
        lo = kind * 64
        return jnp.concatenate([res[2 * h, :, lo:lo + 64], res[2 * h + 1, :, lo:lo + 64]], axis=1)

    def value_t(h):
        return tile(2, h).astype(F32).T.astype(BF16)

    scale_q = jnp.asarray(DK ** (-0.5), BF16)
    gy[y, 0] = tile(0, 0) * scale_q
    gy[y, 1] = tile(1, 1)
    gy[y, 2] = value_t(1)
    gz[z, 0] = tile(0, 1) * scale_q
    gz[z, 1] = tile(1, 0)
    gz[z, 2] = value_t(0)

    def y_dev(yy):
        return {"sp": z * ny + yy}

    def z_dev(zz):
        return {"sp": zz * ny + y}

    g_list = []

    def tile_copy(buf, sent, got, slot, k, dev, way, hop):
        return remote(buf.at[slot, k], buf.at[slot, k], sent.at[way, hop, k], got.at[slot, k], dev)

    def pass_on(hop):
        for k in range(3):
            for buf, sent, got, me, size, dev in (
                (gy, gy_send, gy_recv, y, ny, y_dev), (gz, gz_send, gz_recv, z, nz, z_dev)
            ):
                for side, way in enumerate((1, -1)):
                    def carried(h):
                        return 2 * h < size or (2 * h == size and (k % 2 == 0) == (way == 1))

                    if not (hop > 0 and carried(hop)) and not carried(hop + 1):
                        continue
                    slot = (me + size - way * hop) % size
                    c = tile_copy(buf, sent, got, slot, k, dev((me + size + way) % size), side, hop)
                    if hop > 0 and carried(hop):
                        c.wait_recv()
                    if carried(hop + 1):
                        c.start()
                        g_list.append(c)

    pass_on(0)

    phase("rec_local")
    row = lax.broadcasted_iota(jnp.int32, (ROWS, ROWS), 0)
    col = lax.broadcasted_iota(jnp.int32, (ROWS, ROWS), 1)
    tril = jnp.where(row >= col, 1.0, 0.0).astype(F32)
    rates = []
    scale_col = jnp.broadcast_to(scale_ref[...], (ROWS, ROWS)).T
    for h in range(2):
        rq = tile(3, h).astype(F32)
        rf = tile(4, h).astype(F32)
        ri = tile(5, h)
        edge = lb_ref[h:h + 1, :]
        forget = edge + (1.0 - edge) * jax.nn.sigmoid(rf)
        g = scale_col * jnp.log(forget)
        kk = 1.0 - jnp.exp(g)
        cum = lax.dot_general(
            tril, g, (((1,), (0,)), ((), ())), precision=lax.Precision.HIGHEST, preferred_element_type=F32
        )
        scores = jnp.where(row == col, jnp.sum(rq * kk, axis=-1, keepdims=True), 0.0)
        c8 = cum.reshape(ROWS // 8, 8, DV)
        r8 = lax.broadcasted_iota(jnp.int32, (ROWS // 8, 8, DV), 1)
        for b in (64, 32, 16, 8, 4, 2, 1):
            if b >= 8:
                c3 = cum.reshape(ROWS // (2 * b), 2 * b, DV)
                diff = (c3 - c3[:, b - 1:b, :]).reshape(ROWS, DV)
            else:
                mid = c8[:, b - 1:b, :]
                for first in range(2 * b, 8, 2 * b):
                    mid = jnp.where(r8 >= first, c8[:, first + b - 1:first + b, :], mid)
                diff = (c8 - mid).reshape(ROWS, DV)
            upper = (row & (2 * b - 1)) >= b
            decay = jnp.exp(jnp.where(upper, diff, -diff))
            late = jnp.where(upper, rq * decay, 0.0).astype(BF16)
            early = jnp.where(upper, 0.0, kk * decay).astype(BF16)
            level = dot_nt(late, early)
            scores = scores + jnp.where((row ^ col) < 2 * b, level, 0.0)
        ol_scr[h] = dot_nn(scores.astype(BF16), ri)
        last = cum[ROWS - 1:ROWS, :]
        key_end = (kk * jnp.exp(last - cum)).astype(BF16)
        state_t = dot_nn(ri.astype(F32).T.astype(BF16), key_end)
        qc_scr[h] = (rq * jnp.exp(cum)).astype(BF16)
        st_s[:, h * slice_rows:(h + 1) * slice_rows, :] = state_t.reshape(ny, slice_rows, DV).astype(BF16)
        rates.append(jnp.exp(last))
    packed = pack_rates(*rates)
    for k in range(ny):
        st_s[k, 2 * slice_rows:, :] = packed
    st_r[y] = st_s[y]
    for d in range(1, ny):
        yy = (y + d) % ny
        c = remote(st_s.at[yy], st_r.at[y], st_send.at[d], st_recv.at[y], y_dev(yy))
        c.start()
        g_list.append(c)

    phase("gather_near")
    far_hop = min(3, max(ny, nz) // 2)
    for hop in range(1, far_hop):
        pass_on(hop)
    phase("rec_prefix")
    for d in range(1, ny):
        yy = (y + d) % ny
        remote(st_r.at[yy], st_r.at[yy], st_send.at[0], st_recv.at[yy], y_dev(yy)).wait_recv()
    half = slice_rows

    def step_of(ref):
        d0, d1 = unpack_rates(ref[2 * half:, :])
        return d0, ref[0:half, :].astype(F32), d1, ref[half:2 * half, :].astype(F32)

    s0 = s1 = jnp.zeros((half, DV), F32)
    c0 = c1 = jnp.ones((1, DV), F32)
    for k in range(ny):
        pref[k, 0:half, :] = s0
        pref[k, half:2 * half, :] = s1
        pref[k, 2 * half:2 * half + 8, :] = jnp.broadcast_to(c0, (8, DV))
        pref[k, 2 * half + 8:2 * half + 16, :] = jnp.broadcast_to(c1, (8, DV))
        d0, a0, d1, a1 = step_of(st_r.at[k])
        s0, s1, c0, c1 = d0 * s0 + a0, d1 * s1 + a1, c0 * d0, c1 * d1
    tot_s[0:half, :] = s0.astype(BF16)
    tot_s[half:2 * half, :] = s1.astype(BF16)
    tot_s[2 * half:, :] = pack_rates(c0, c1)
    for d in range(1, nz):
        zz = (z + d) % nz
        c = remote(tot_s, tot_r.at[z], tot_send.at[d], tot_recv.at[z], z_dev(zz))
        c.start()
        g_list.append(c)

    phase("rec_totals")
    for d in range(1, nz):
        zz = (z + d) % nz
        remote(tot_r.at[zz], tot_r.at[zz], tot_send.at[0], tot_recv.at[zz], z_dev(zz)).wait_recv()

    def fold(k, carry):
        d0, a0, d1, a1 = step_of(tot_r.at[k])
        return (d0 * carry[0] + a0, d1 * carry[1] + a1)

    entry = lax.fori_loop(0, z, fold, (jnp.zeros((half, DV), F32), jnp.zeros((half, DV), F32)))
    for k in range(ny):
        for h in range(2):
            d = pref[k, 2 * half + 8 * h:2 * half + 8 * h + 1, :]
            in_s[k, h] = (d * entry[h] + pref[k, h * half:(h + 1) * half, :]).astype(BF16)
    in_r[y] = in_s[y]
    for d in range(1, ny):
        yy = (y + d) % ny
        c = remote(in_s.at[yy], in_r.at[y], in_send.at[d], in_recv.at[y], y_dev(yy))
        c.start()
        g_list.append(c)

    phase("gather_wait")
    for hop in range(far_hop, max(ny, nz) // 2 + 1):
        pass_on(hop)

    phase("att_head0")
    lane = lax.broadcasted_iota(jnp.int32, (ROWS, DV), 1)

    def unit(queries, tiles, count, limits, masked_from, o_out, t_out, lane_slot):
        zero = jnp.zeros_like(queries)
        both = jnp.concatenate(
            [jnp.where(lane < DK, queries, zero), jnp.where(lane < DK, zero, queries)], axis=0
        )
        keys = count * ROWS
        s_scr[lane_slot, :keys, :] = dot_nt(tiles[:count, 1].reshape(keys, DV), both)
        top = jnp.full((8, 2 * ROWS), NEG, F32)
        for k in range(count):
            rows = slice(k * ROWS, (k + 1) * ROWS)
            s = s_scr[lane_slot, rows, :]
            if k >= masked_from:
                ri_ = lax.broadcasted_iota(jnp.int32, (ROWS, 2 * ROWS), 0)
                ci_ = lax.broadcasted_iota(jnp.int32, (ROWS, 2 * ROWS), 1) & (ROWS - 1)
                s = jnp.where(ri_ - ci_ <= limits(k), s, NEG)
                s_scr[lane_slot, rows, :] = s
            top = jnp.maximum(top, jnp.max(s.reshape(ROWS // 8, 8, 2 * ROWS), axis=0))
        top = jnp.max(top, axis=0, keepdims=True)
        total = jnp.zeros((8, 2 * ROWS), F32)
        for k in range(count):
            rows = slice(k * ROWS, (k + 1) * ROWS)
            e = jnp.exp(s_scr[lane_slot, rows, :] - top)
            total = total + jnp.sum(e.reshape(ROWS // 8, 8, 2 * ROWS), axis=0)
            e_scr[lane_slot, rows, :] = e.astype(BF16)
        num = dot_nn(vt[:, :keys], e_scr[lane_slot, :keys, :])
        o_out[...] = num.astype(BF16)
        t_out[0:1, :] = top
        t_out[1:2, :] = jnp.sum(total, axis=0, keepdims=True)

    def head0(count):
        for k in range(count):
            vt[:, k * ROWS:(k + 1) * ROWS] = gz[k, 2]

        def body(i, carry):
            blocks = [(y + ny // 2 + i) % ny, (y + 2 * ny - 1 - i - ny // 2) % ny]
            for j, yq in enumerate(blocks):
                unit(
                    gy[yq, 0], gz, count,
                    lambda k, yq=yq: ((z - k) * ny + (yq - y)) * ROWS,
                    count - 2, o0s.at[yq], t0s.at[yq], j,
                )
            for yq in blocks:
                @pl.when(yq != y)
                def _():
                    remote(o0s.at[yq], o0r.at[y], o0_send.at[yq], o0_recv.at[y], y_dev(yq)).start()
                    remote(t0s.at[yq], t0r.at[y], t0_send.at[yq], t0_recv.at[y], y_dev(yq)).start()

            return carry

        lax.fori_loop(0, ny // 2, body, 0)

    for count in range(2, nz + 1, 2):
        pl.when(z // 2 == count // 2 - 1)(functools.partial(head0, count))
    o0r[y] = o0s[y]
    t0r[y] = t0s[y]

    phase("att_head1")
    for k in range(ny):
        vt[:, k * ROWS:(k + 1) * ROWS] = gy[k, 2]

    def head1(i, carry):
        zq = nz - 1 - i
        unit(gz[zq, 0], gy, ny, lambda k: 0, ny, o1s.at[zq], t1s.at[zq], 0)
        remote(o1s.at[zq], o1r.at[z], o1_send.at[zq], o1_recv.at[z], z_dev(zq)).start()
        remote(t1s.at[zq], t1r.at[z], t1_send.at[zq], t1_recv.at[z], z_dev(zq)).start()
        return carry

    lax.fori_loop(0, nz - 1 - z, head1, 0)
    unit(gz[z, 0], gy, ny, lambda k: (y - k) * ROWS, 0, o1r.at[z], t1r.at[z], 0)

    phase("rec_result")
    for d in range(1, ny):
        yy = (y + d) % ny
        remote(in_r.at[yy], in_r.at[yy], in_send.at[0], in_recv.at[yy], y_dev(yy)).wait_recv()
    rec = []
    for h in range(2):
        o = ol_scr[h] + dot_nt(qc_scr[h], in_r[:, h].reshape(DV, DV))
        rec.append(norm_rows(o, recg_ref[...]).astype(BF16))
    rec_rows = jnp.concatenate(rec, axis=1)

    phase("merge_start")
    def merge(o_ref, t_ref, k, carry):
        top, total, num = carry
        t_new = t_ref[k]
        now = jnp.maximum(top, t_new[0:1, :])
        old_w = jnp.exp(top - now)
        new_w = jnp.exp(t_new[0:1, :] - now)
        total = old_w * total + new_w * t_new[1:2, :]
        num = old_w * num + new_w * o_ref[k].astype(F32)
        return (now, total, num)

    start = (
        jnp.full((1, 2 * ROWS), NEG, F32), jnp.zeros((1, 2 * ROWS), F32), jnp.zeros((DV, 2 * ROWS), F32)
    )

    def finish(h, carry):
        top, total, num = carry
        att = num[:, :ROWS] / total[:, :ROWS] - lam_ref[h] * num[:, ROWS:] / total[:, ROWS:]
        att = att * lax.rsqrt(jnp.mean(att * att, axis=0, keepdims=True) + EPS)
        lws_ref[h:h + 1, :] = top[:, :ROWS] + jnp.log(total[:, :ROWS])
        return (att.T * attg_ref[...] * 0.8).astype(BF16)

    def merge0(k, carry):
        @pl.when(k != y)
        def _():
            remote(o0r.at[k], o0r.at[k], o0_send.at[0], o0_recv.at[k], y_dev(y)).wait_recv()
            remote(t0r.at[k], t0r.at[k], t0_send.at[0], t0_recv.at[k], y_dev(y)).wait_recv()

        return merge(o0r, t0r, k, carry)

    def merge1(k, carry):
        @pl.when(k != z)
        def _():
            remote(o1r.at[k], o1r.at[k], o1_send.at[0], o1_recv.at[k], z_dev(z)).wait_recv()
            remote(t1r.at[k], t1r.at[k], t1_send.at[0], t1_recv.at[k], z_dev(z)).wait_recv()

        return merge(o1r, t1r, k, carry)

    phase("merge_zero")
    att0 = finish(0, lax.fori_loop(0, ny, merge0, start))
    phase("merge_one")
    att1 = finish(1, lax.fori_loop(0, z + 1, merge1, start))
    att_rows = jnp.concatenate([att0, att1], axis=1)

    phase("project_out")
    for c in wo_copies:
        c.wait()
    width = wo.shape[2] // PARTS
    p_list = []
    for k in range(PARTS):
        cols = slice(k * width, (k + 1) * width)
        part = dot_nn(att_rows, wo[0, :, cols]) + dot_nn(rec_rows, wo[1, :, cols])
        pbuf[k] = part.astype(BF16)
        c = remote(pbuf.at[k], prx.at[k], p_send.at[k], p_recv.at[k], {"tp": t_other})
        c.start()
        p_list.append(c)
    for k in range(PARTS):
        p_list[k].wait_recv()
        out_ref[:, k * width:(k + 1) * width] = (pbuf[k].astype(F32) + prx[k].astype(F32)).astype(BF16)

    phase("drain")
    for c in a_list + r_list + g_list + p_list:
        c.wait_send()

    def sent0(k, carry):
        @pl.when(k != y)
        def _():
            remote(o0s.at[k], o0r.at[y], o0_send.at[k], o0_recv.at[y], y_dev(k)).wait_send()
            remote(t0s.at[k], t0r.at[y], t0_send.at[k], t0_recv.at[y], y_dev(k)).wait_send()

        return carry

    lax.fori_loop(0, ny, sent0, 0)

    def sent1(k, carry):
        remote(o1s.at[k], o1r.at[z], o1_send.at[k], o1_recv.at[z], z_dev(k)).wait_send()
        remote(t1s.at[k], t1r.at[z], t1_send.at[k], t1_recv.at[z], z_dev(k)).wait_send()
        return carry

    lax.fori_loop(z + 1, nz, sent1, 0)
    phase(None)


def hand_over(mixed_ref, log_ref, mixed_out, log_out):
    mixed_out[...] = mixed_ref[...]
    log_out[...] = log_ref[...]


def on_device(nz, ny, tokens, in_gain, wq, wk, wv, wrq, wrf, wri, lam, lb, scale, attg, recg, wa, wr):
    d = tokens.shape[1]
    out_cols = wa.shape[1]
    any_spec = pl.BlockSpec(memory_space=pl.ANY)
    vmem = pl.BlockSpec(memory_space=pltpu.VMEM)
    smem = pl.BlockSpec(memory_space=pltpu.SMEM)
    slice_rows = DV // ny
    st_rows = 2 * slice_rows + 16
    dma = pltpu.SemaphoreType.DMA
    scratch = [
        pltpu.VMEM((ROWS, d), BF16),
        pltpu.VMEM((COLS, d), BF16),
        pltpu.VMEM((2, wa.shape[0], out_cols), BF16),
        pltpu.VMEM((FS, ROWS, d), BF16),
        pltpu.VMEM((FS, ROWS, COLS), BF16),
        pltpu.VMEM((3, ROWS, COLS), BF16),
        pltpu.VMEM((ny, 3, ROWS, DV), BF16),
        pltpu.VMEM((nz, 3, ROWS, DV), BF16),
        pltpu.VMEM((2, max(ny, nz) * ROWS, 2 * ROWS), F32),
        pltpu.VMEM((2, max(ny, nz) * ROWS, 2 * ROWS), BF16),
        pltpu.VMEM((DV, max(ny, nz) * ROWS), BF16),
        pltpu.VMEM((ny, DV, 2 * ROWS), BF16),
        pltpu.VMEM((ny, DV, 2 * ROWS), BF16),
        pltpu.VMEM((ny, 8, 2 * ROWS), F32),
        pltpu.VMEM((ny, 8, 2 * ROWS), F32),
        pltpu.VMEM((nz, DV, 2 * ROWS), BF16),
        pltpu.VMEM((nz, DV, 2 * ROWS), BF16),
        pltpu.VMEM((nz, 8, 2 * ROWS), F32),
        pltpu.VMEM((nz, 8, 2 * ROWS), F32),
        pltpu.VMEM((ny, st_rows, DV), BF16),
        pltpu.VMEM((ny, st_rows, DV), BF16),
        pltpu.VMEM((st_rows, DV), BF16),
        pltpu.VMEM((nz, st_rows, DV), BF16),
        pltpu.VMEM((ny, 2, slice_rows, DV), BF16),
        pltpu.VMEM((ny, 2, slice_rows, DV), BF16),
        pltpu.VMEM((ny, st_rows, DV), F32),
        pltpu.VMEM((2, ROWS, DV), BF16),
        pltpu.VMEM((2, ROWS, DV), F32),
        pltpu.VMEM((PARTS, ROWS, out_cols // PARTS), BF16),
        pltpu.VMEM((PARTS, ROWS, out_cols // PARTS), BF16),
        dma((9,)), dma((12,)), dma((FS, 4)), dma((3,)), dma((FS,)),
        dma((2, ny // 2 + 1, 3)), dma((ny, 3)), dma((2, nz // 2 + 1, 3)), dma((nz, 3)),
        dma((ny,)), dma((ny,)), dma((ny,)), dma((ny,)),
        dma((nz,)), dma((nz,)), dma((nz,)), dma((nz,)),
        dma((ny,)), dma((ny,)), dma((nz,)), dma((nz,)), dma((ny,)), dma((ny,)),
        dma((PARTS,)), dma((PARTS,)),
    ]
    mixed, log_sum = pl.pallas_call(
        functools.partial(kernel_body, nz, ny),
        out_shape=(
            jax.ShapeDtypeStruct((ROWS, out_cols), BF16),
            jax.ShapeDtypeStruct((2, ROWS), F32),
        ),
        in_specs=[any_spec, vmem] + [any_spec] * 6 + [smem, vmem, vmem, vmem, vmem, any_spec, any_spec],
        out_specs=(vmem, vmem),
        scratch_shapes=scratch,
        compiler_params=pltpu.CompilerParams(
            collective_id=0, has_side_effects=True, vmem_limit_bytes=56 * 1024 * 1024
        ),
    )(
        tokens, in_gain.reshape(1, d), wq.T, wk.T, wv.T, wrq.T, wrf.T, wri.T, lam, lb,
        scale.reshape(1, ROWS), attg.reshape(1, DV), recg.reshape(1, DV), wa, wr,
    )
    return pl.pallas_call(
        hand_over,
        out_shape=(
            jax.ShapeDtypeStruct((ROWS, out_cols), BF16),
            jax.ShapeDtypeStruct((2, ROWS), F32),
        ),
        in_specs=[vmem, vmem],
        out_specs=(vmem, vmem),
    )(mixed, log_sum)


def solution(mesh):
    sp = mesh.shape["sp"]
    nz = 1
    while nz * nz < sp:
        nz *= 2
    ny = sp // nz
    col_split = P(None, ("tp", "fs"))
    placed = (
        P(("fs", "sp"), None), P(),
        col_split, col_split, col_split, col_split, col_split, col_split,
        P("tp"), P("tp", None), P(("fs", "sp")), P(), P(),
        P("tp", None), P("tp", None),
    )
    return jax.shard_map(
        functools.partial(on_device, nz, ny),
        mesh=mesh,
        in_specs=placed,
        out_specs=(P(("fs", "sp"), None), P("tp", ("fs", "sp"))),
        check_vma=False,
    )
```

```python
import functools

import jax
import jax.numpy as jnp
from jax import lax
from jax.experimental import pallas as pl
from jax.experimental.pallas import tpu as pltpu
from jax.sharding import PartitionSpec as P

DK = 64
DV = 128
ROWS = 128
COLS = 384
FIRST = 256
EPS = 1e-06
NEG = -1e30
FS = 4
PARTS = 4
MESH = pl.DeviceIdType.MESH
F32 = jnp.float32
BF16 = jnp.bfloat16


def dot_nn(a, b):
    return lax.dot_general(a, b, (((1,), (0,)), ((), ())), preferred_element_type=F32)


def dot_nt(a, b):
    return lax.dot_general(a, b, (((1,), (1,)), ((), ())), preferred_element_type=F32)


def pack_rates(first, second):
    parts = []
    for rate in (first, second):
        high = rate.astype(BF16).astype(F32)
        parts += [jnp.broadcast_to(v, (4, DV)) for v in (high, rate - high)]
    return jnp.concatenate(parts, axis=0).astype(BF16)


def unpack_rates(packed):
    wide = packed.astype(F32)
    return wide[0:1] + wide[4:5], wide[8:9] + wide[12:13]


def pack_stats(rows):
    tile = jnp.zeros((16, DV), F32)
    where = lax.broadcasted_iota(jnp.int32, (16, DV), 0)
    for i, value in enumerate(rows):
        high = value.astype(BF16).astype(F32)
        middle = (value - high).astype(BF16).astype(F32)
        for j, part in enumerate((high, middle, value - high - middle)):
            tile = jnp.where(where == 3 * i + j, part, tile)
    return tile.astype(BF16)


def unpack_stats(packed):
    wide = packed.astype(F32)
    return [wide[3 * i:3 * i + 1] + wide[3 * i + 1:3 * i + 2] + wide[3 * i + 2:3 * i + 3] for i in range(4)]


def norm_rows(values, gain):
    mean = jnp.mean(values * values, axis=-1, keepdims=True)
    return values * lax.rsqrt(mean + EPS) * gain


def kernel_body(
    nz, ny,
    tok_hbm, gain_ref, wq, wk, wv, wrq, wrf, wri, lam_ref, lb_ref, scale_ref, attg_ref, recg_ref,
    wa_hbm, wr_hbm,
    out_ref, lws_ref,
    tok, wcat, wo, nrm, res, res2, rsend, rsend2,
    gy, gz, acc, stat, qb, po_s, po_r,
    st_s, st_r, tot_s, tot_r, in_s, in_r, pref, qc_scr, ol_scr,
    pbuf, prx,
    lsem, a_send, a_recv, r_send, r_recv,
    gy_send, gy_recv, gz_send, gz_recv,
    po_send, po_recv,
    st_send, st_recv, tot_send, tot_recv, in_send, in_recv,
    p_send, p_recv,
):
    p = lax.axis_index("sp")
    x = lax.axis_index("fs")
    t = lax.axis_index("tp")
    z = p // ny
    y = p % ny
    t_other = 1 - t
    xl = (x + 3) % 4
    xr = (x + 1) % 4
    xo = (x + 2) % 4
    slice_rows = DV // ny

    open_scope = []

    def phase(name):
        if open_scope:
            open_scope.pop().__exit__(None, None, None)
        if name:
            scope = jax.named_scope(name)
            scope.__enter__()
            open_scope.append(scope)

    phase("start")
    weights = (wq, wk, wv, wrq, wrf, wri)
    tok_copy = pltpu.make_async_copy(tok_hbm, tok, lsem.at[0])
    tok_copy.start()
    w_copies = [
        pltpu.make_async_copy(w, wcat.at[pl.ds(i * DK, DK)], lsem.at[1 + i]) for i, w in enumerate(weights)
    ]
    for c in w_copies:
        c.start()
    wo_copies = [
        pltpu.make_async_copy(wa_hbm, wo.at[0], lsem.at[7]),
        pltpu.make_async_copy(wr_hbm, wo.at[1], lsem.at[8]),
    ]
    for c in wo_copies:
        c.start()

    barrier = pltpu.get_barrier_semaphore()

    def greet(dev):
        pl.semaphore_signal(barrier, inc=1, device_id=dev, device_id_type=MESH)

    greet({"tp": t_other})
    for d in range(1, 4):
        greet({"fs": (x + d) % 4})
    for d in range(1, ny):
        greet({"sp": z * ny + (y + d) % ny})
    for d in range(1, nz):
        greet({"sp": ((z + d) % nz) * ny + y})

    def remote(src, dst, ssem, rsem, dev):
        return pltpu.make_async_remote_copy(
            src_ref=src, dst_ref=dst, send_sem=ssem, recv_sem=rsem, device_id=dev, device_id_type=MESH
        )

    def piece(f, tt, pc):
        return nrm.at[f, pl.ds(pl.multiple_of(tt * 64 + pc * 32, 32), 32)]

    def a_sem(f, tt, pc):
        return a_recv.at[f, tt * 2 + pc]

    def normalise(tt, pc):
        rows = pl.ds(pl.multiple_of(tt * 64 + pc * 32, 32), 32)
        nrm[x, rows, :] = norm_rows(tok[rows, :].astype(F32), gain_ref[...]).astype(BF16)

    acc[...] = jnp.zeros_like(acc)
    stat[...] = jnp.full(stat.shape, NEG, F32)
    tok_copy.wait()
    normalise(t, 0)
    normalise(t, 1)
    phase("entry_barrier")
    pl.semaphore_wait(barrier, 1 + 3 + (ny - 1) + (nz - 1))

    a_list = []

    def a_start(k, f, pc, dev):
        c = remote(piece(f, t, pc), piece(f, t, pc), a_send.at[k], a_sem(f, t, pc), dev)
        c.start()
        a_list.append(c)

    def a_wait(f, tt, pc):
        remote(piece(f, tt, pc), piece(f, tt, pc), a_send.at[0], a_sem(f, tt, pc), {"fs": xr}).wait_recv()

    phase("x_own")
    a_start(0, x, 0, {"fs": xr})
    a_start(1, x, 1, {"fs": xl})
    a_start(2, x, 1, {"fs": xr})
    a_start(3, x, 0, {"fs": xl})
    normalise(t_other, 0)
    normalise(t_other, 1)
    for i in range(6):
        w_copies[i].wait()

    def project(rows):
        return dot_nt(rows, wcat[...]).astype(BF16)

    own = project(nrm[x])
    res[x] = own[:, :FIRST]
    res2[x] = own[:, FIRST:]
    phase("x_forward")
    a_wait(xl, t, 0)
    a_start(4, xl, 0, {"fs": xr})
    a_start(5, xl, 0, {"tp": t_other})
    a_wait(xr, t, 1)
    a_start(6, xr, 1, {"fs": xl})
    a_start(7, xr, 1, {"tp": t_other})
    a_wait(xl, t, 1)
    a_start(8, xl, 1, {"tp": t_other})
    a_wait(xr, t, 0)
    a_start(9, xr, 0, {"tp": t_other})

    r_list = []

    def answer(k, f):
        for j, (out, into) in enumerate(((rsend, res), (rsend2, res2))):
            c = remote(out.at[k], into.at[x], r_send.at[k, j], r_recv.at[x, j], {"fs": f})
            c.start()
            r_list.append(c)

    phase("x_near")
    for f in (xl, xr):
        a_wait(f, t_other, 0)
        a_wait(f, t_other, 1)
    near = project(jnp.concatenate([nrm[xl], nrm[xr]], axis=0))
    for k in (0, 1):
        rsend[k] = near[k * ROWS:(k + 1) * ROWS, :FIRST]
        rsend2[k] = near[k * ROWS:(k + 1) * ROWS, FIRST:]
    answer(0, xl)
    answer(1, xr)
    phase("x_far")
    a_wait(xo, t, 0)
    a_start(10, xo, 0, {"tp": t_other})
    a_wait(xo, t, 1)
    a_start(11, xo, 1, {"tp": t_other})
    a_wait(xo, t_other, 0)
    a_wait(xo, t_other, 1)
    far = project(nrm[xo])
    rsend[2] = far[:, :FIRST]
    rsend2[2] = far[:, FIRST:]
    answer(2, xo)
    phase("x_answers")
    for f in (xl, xr, xo):
        remote(res.at[f], res.at[f], r_send.at[0, 0], r_recv.at[f, 0], {"fs": xr}).wait_recv()

    phase("tiles")
    def tile(kind, h):
        lo, ref = (kind * DK, res) if kind * DK < FIRST else (kind * DK - FIRST, res2)
        return jnp.concatenate([ref[2 * h, :, lo:lo + DK], ref[2 * h + 1, :, lo:lo + DK]], axis=1)

    def value_t(h):
        return tile(2, h).astype(F32).T.astype(BF16)

    scale_q = jnp.asarray(DK ** (-0.5), BF16)
    gy[0, 0] = (tile(0, 0) * scale_q).astype(F32).T.astype(BF16)
    gy[0, 1] = tile(1, 1)
    gy[0, 2] = value_t(1)
    gz[0, 0] = (tile(0, 1) * scale_q).astype(F32).T.astype(BF16)
    gz[0, 1] = tile(1, 0)
    gz[0, 2] = value_t(0)

    def y_dev(yy):
        return {"sp": z * ny + yy}

    def z_dev(zz):
        return {"sp": zz * ny + y}

    g_list = []

    def pass_on(hop):
        for k in range(3):
            for buf, sent, got, me, size, dev in (
                (gy, gy_send, gy_recv, y, ny, y_dev), (gz, gz_send, gz_recv, z, nz, z_dev)
            ):
                for side, way in enumerate((1, -1)):
                    def carried(h):
                        return 2 * h < size or (2 * h == size and (k % 2 == 0) == (way == 1))

                    here = (-way * hop) % size
                    there = (-way * (hop + 1)) % size
                    dev_next = dev((me + size + way) % size)
                    if hop > 0 and carried(hop):
                        remote(buf.at[here, k], buf.at[here, k], sent.at[0, 0, 0], got.at[here, k], dev_next).wait_recv()
                    if carried(hop + 1):
                        c = remote(buf.at[here, k], buf.at[there, k], sent.at[side, hop, k], got.at[there, k], dev_next)
                        c.start()
                        g_list.append(c)

    pass_on(0)

    phase("rec_local")
    for f in (xl, xr, xo):
        remote(res2.at[f], res2.at[f], r_send.at[0, 1], r_recv.at[f, 1], {"fs": xr}).wait_recv()
    row = lax.broadcasted_iota(jnp.int32, (ROWS, ROWS), 0)
    col = lax.broadcasted_iota(jnp.int32, (ROWS, ROWS), 1)
    tril = jnp.where(row >= col, 1.0, 0.0).astype(F32)
    rates = []
    scale_col = jnp.broadcast_to(scale_ref[...], (ROWS, ROWS)).T
    for h in range(2):
        rq = tile(3, h).astype(F32)
        rf = tile(4, h).astype(F32)
        ri = tile(5, h)
        edge = lb_ref[h:h + 1, :]
        forget = edge + (1.0 - edge) * jax.nn.sigmoid(rf)
        g = scale_col * jnp.log(forget)
        kk = 1.0 - jnp.exp(g)
        cum = lax.dot_general(
            tril, g, (((1,), (0,)), ((), ())), precision=lax.Precision.HIGHEST, preferred_element_type=F32
        )
        scores = jnp.where(row == col, jnp.sum(rq * kk, axis=-1, keepdims=True), 0.0)
        c8 = cum.reshape(ROWS // 8, 8, DV)
        r8 = lax.broadcasted_iota(jnp.int32, (ROWS // 8, 8, DV), 1)
        for b in (64, 32, 16, 8, 4, 2, 1):
            if b >= 8:
                c3 = cum.reshape(ROWS // (2 * b), 2 * b, DV)
                diff = (c3 - c3[:, b - 1:b, :]).reshape(ROWS, DV)
            else:
                mid = c8[:, b - 1:b, :]
                for first in range(2 * b, 8, 2 * b):
                    mid = jnp.where(r8 >= first, c8[:, first + b - 1:first + b, :], mid)
                diff = (c8 - mid).reshape(ROWS, DV)
            upper = (row & (2 * b - 1)) >= b
            decay = jnp.exp(jnp.where(upper, diff, -diff))
            late = jnp.where(upper, rq * decay, 0.0).astype(BF16)
            early = jnp.where(upper, 0.0, kk * decay).astype(BF16)
            level = dot_nt(late, early)
            scores = scores + jnp.where((row ^ col) < 2 * b, level, 0.0)
        ol_scr[h] = dot_nn(scores.astype(BF16), ri)
        last = cum[ROWS - 1:ROWS, :]
        key_end = (kk * jnp.exp(last - cum)).astype(BF16)
        state_t = dot_nn(ri.astype(F32).T.astype(BF16), key_end)
        qc_scr[h] = (rq * jnp.exp(cum)).astype(BF16)
        st_s[:, h * slice_rows:(h + 1) * slice_rows, :] = state_t.reshape(ny, slice_rows, DV).astype(BF16)
        rates.append(jnp.exp(last))
    packed = pack_rates(*rates)
    for k in range(ny):
        st_s[k, 2 * slice_rows:, :] = packed
    def state_send():
        st_r[y] = st_s[y]
        for d in range(1, ny):
            yy = (y + d) % ny
            c = remote(st_s.at[yy], st_r.at[y], st_send.at[d], st_recv.at[y], y_dev(yy))
            c.start()
            g_list.append(c)

    half = slice_rows

    def step_of(ref):
        d0, d1 = unpack_rates(ref[2 * half:, :])
        return d0, ref[0:half, :].astype(F32), d1, ref[half:2 * half, :].astype(F32)

    def state_prefix():
        phase("rec_prefix")
        for d in range(1, ny):
            yy = (y + d) % ny
            remote(st_r.at[yy], st_r.at[yy], st_send.at[0], st_recv.at[yy], y_dev(yy)).wait_recv()

        s0 = s1 = jnp.zeros((half, DV), F32)
        c0 = c1 = jnp.ones((1, DV), F32)
        for k in range(ny):
            pref[k, 0:half, :] = s0
            pref[k, half:2 * half, :] = s1
            pref[k, 2 * half:2 * half + 8, :] = jnp.broadcast_to(c0, (8, DV))
            pref[k, 2 * half + 8:2 * half + 16, :] = jnp.broadcast_to(c1, (8, DV))
            d0, a0, d1, a1 = step_of(st_r.at[k])
            s0, s1, c0, c1 = d0 * s0 + a0, d1 * s1 + a1, c0 * d0, c1 * d1
        tot_s[0:half, :] = s0.astype(BF16)
        tot_s[half:2 * half, :] = s1.astype(BF16)
        tot_s[2 * half:, :] = pack_rates(c0, c1)
        for d in range(1, nz):
            zz = (z + d) % nz
            c = remote(tot_s, tot_r.at[z], tot_send.at[d], tot_recv.at[z], z_dev(zz))
            c.start()
            g_list.append(c)

    def state_entry():
        phase("rec_totals")
        for d in range(1, nz):
            zz = (z + d) % nz
            remote(tot_r.at[zz], tot_r.at[zz], tot_send.at[0], tot_recv.at[zz], z_dev(zz)).wait_recv()

        def fold(k, carry):
            d0, a0, d1, a1 = step_of(tot_r.at[k])
            return (d0 * carry[0] + a0, d1 * carry[1] + a1)

        entry = lax.fori_loop(0, z, fold, (jnp.zeros((half, DV), F32), jnp.zeros((half, DV), F32)))
        for k in range(ny):
            for h in range(2):
                d = pref[k, 2 * half + 8 * h:2 * half + 8 * h + 1, :]
                in_s[k, h] = (d * entry[h] + pref[k, h * half:(h + 1) * half, :]).astype(BF16)
        in_r[y] = in_s[y]
        for d in range(1, ny):
            yy = (y + d) % ny
            c = remote(in_s.at[yy], in_r.at[y], in_send.at[d], in_recv.at[y], y_dev(yy))
            c.start()
            g_list.append(c)

    channel = lax.broadcasted_iota(jnp.int32, (ROWS, DV), 0)
    below = (
        lax.broadcasted_iota(jnp.int32, (ROWS, 2 * ROWS), 0)
        <= (lax.broadcasted_iota(jnp.int32, (ROWS, 2 * ROWS), 1) & (ROWS - 1))
    )

    def seen(head, off):
        if off % nz == 0:
            return None
        other = (z + off % nz) % nz
        return other < z if head == 0 else other > z

    def when(condition, body):
        if condition is None:
            body()
        else:
            pl.when(condition)(body)

    def ring(hop, size):
        if hop == 0:
            return [0]
        if 2 * hop < size:
            return [hop, -hop]
        return [hop] if 2 * hop == size else []

    def within(hop, size):
        return [o for h in range(hop + 1) for o in ring(h, size)]

    def arrival(off, size):
        return [o % size for o in within(size, size)].index(off % size)

    def sides(head):
        return (gy, gz, ny, nz) if head == 0 else (gz, gy, nz, ny)

    def keep_queries(head, off):
        q_buf, _, q_size, _ = sides(head)
        queries = q_buf[off % q_size, 0]
        zero = jnp.zeros_like(queries)
        at = arrival(off, q_size) * 2 * ROWS
        qb[head, :, at:at + ROWS] = jnp.where(channel < DK, queries, zero)
        qb[head, :, at + ROWS:at + 2 * ROWS] = jnp.where(channel < DK, zero, queries)

    def hidden(head, q_off, k_off):
        _, _, q_size, k_size = sides(head)
        if head == 0:
            if k_off % nz == 0:
                return y > (y + q_off % ny) % ny
            return (z + k_off % nz) % nz > z
        if q_off % nz == 0:
            return (y + k_off % ny) % ny > y
        return (z + q_off % nz) % nz < z

    def attend(head, q_offs, k_offs, checked=True):
        _, kv_buf, q_size, k_size = sides(head)
        if not q_offs or not k_offs:
            return
        lo = arrival(q_offs[0], q_size) * 2 * ROWS
        hi = lo + len(q_offs) * 2 * ROWS
        slots = [o % k_size for o in k_offs]
        s = dot_nn(jnp.concatenate([kv_buf[i, 1] for i in slots], axis=0), qb[head, :, lo:hi])
        parts = []
        for i, k_off in enumerate(k_offs):
            part = s[i * ROWS:(i + 1) * ROWS]
            blocks = []
            for j, q_off in enumerate(q_offs):
                block = part[:, j * 2 * ROWS:(j + 1) * 2 * ROWS]
                if q_off % q_size == 0 and k_off % k_size == 0:
                    block = jnp.where(below, block, NEG)
                elif checked or (k_off if head == 0 else q_off) % nz == 0:
                    block = block + jnp.where(hidden(head, q_off, k_off), NEG, 0.0).astype(F32)
                blocks.append(block)
            parts.append(jnp.concatenate(blocks, axis=1))
        width = hi - lo
        best = jnp.max(functools.reduce(jnp.maximum, parts).reshape(ROWS // 8, 8, width), axis=0)
        top = stat[head, 0:1, lo:hi]
        now = jnp.maximum(top, jnp.max(best, axis=0, keepdims=True))
        es = [jnp.exp(part - now) for part in parts]
        summed = functools.reduce(jnp.add, [jnp.sum(e.reshape(ROWS // 8, 8, width), axis=0) for e in es])
        new = dot_nn(
            jnp.concatenate([kv_buf[i, 2] for i in slots], axis=1),
            jnp.concatenate([e.astype(BF16) for e in es], axis=0),
        )
        keep = jnp.exp(top - now)
        stat[head, 0:1, lo:hi] = now
        stat[head, 1:2, lo:hi] = keep * stat[head, 1:2, lo:hi] + jnp.sum(summed, axis=0, keepdims=True)
        acc[head, :, lo:hi] = keep * acc[head, :, lo:hi] + new

    def early(hop):
        queries, keys = within(hop, ny), within(hop, nz)
        for k in keys:
            when(seen(0, k), lambda k=k: attend(0, queries, [k], False))
        queries, keys = within(hop, nz), within(hop, ny)
        for q in queries:
            when(seen(1, q), lambda q=q: attend(1, [q], keys, False))

    def late_queries(hop):
        keys = within(hop, nz)
        attend(0, ring(hop, ny), [k for k in keys if k <= 0])
        rest = [k for k in keys if k > 0]
        if rest and ring(hop, ny):
            pl.when(z + max(rest) >= nz)(lambda: attend(0, ring(hop, ny), rest))
        for q in ring(hop, nz):
            when(seen(1, q), lambda q=q: attend(1, [q], within(hop, ny), False))

    def late_keys(hop):
        for k in ring(hop, nz):
            when(seen(0, k), lambda k=k: attend(0, within(hop - 1, ny), [k], False))
        attend(1, within(hop - 1, nz), ring(hop, ny))

    rings = ((0, y, ny, y_dev), (1, z, nz, z_dev))

    def load_own(head, off, size):
        lo = arrival(off, size) * 2 * ROWS
        hi = lo + 2 * ROWS
        return stat[head, 0:1, lo:hi], stat[head, 1:2, lo:hi], acc[head, :, lo:hi]

    def combine(one, message):
        top, total, num = one
        t0, l0, t1, l1 = unpack_stats(message[2 * DV:, :])
        new_top = jnp.concatenate([t0, t1], axis=1)
        now = jnp.maximum(top, new_top)
        keep = jnp.exp(top - now)
        weight = jnp.exp(new_top - now)
        new_num = jnp.concatenate([message[0:DV, :].astype(F32), message[DV:2 * DV, :].astype(F32)], axis=1)
        total = keep * total + weight * jnp.concatenate([l0, l1], axis=1)
        return now, total, keep * num + weight * new_num

    def send_partial(head, side, dist, value, me, size, dev):
        way = -1 if side == 0 else 1
        top, total, num = value
        out = po_s.at[head, side, dist]
        out[0:DV, :] = num[:, :ROWS].astype(BF16)
        out[DV:2 * DV, :] = num[:, ROWS:].astype(BF16)
        out[2 * DV:, :] = pack_stats([top[:, :ROWS], total[:, :ROWS], top[:, ROWS:], total[:, ROWS:]])
        step = dist if dist <= 2 else 1
        c = remote(
            out, po_r.at[head, side, dist], po_send.at[head, side, dist], po_recv.at[head, side, dist],
            dev((me + size + way * step) % size),
        )
        c.start()
        g_list.append(c)

    def await_partial(head, side, dist, dev, me):
        remote(
            po_r.at[head, side, dist], po_r.at[head, side, dist],
            po_send.at[head, side, dist], po_recv.at[head, side, dist], dev(me),
        ).wait_recv()
        return po_r.at[head, side, dist]

    def reach(side, size):
        return size // 2 if side == 0 else (size - 1) // 2

    def own_part(head, side, dist, me, size, dev):
        way = -1 if side == 0 else 1
        send_partial(head, side, dist, load_own(head, way * dist, size), me, size, dev)

    def passing(head, side, dist, me, size, dev):
        way = -1 if side == 0 else 1
        got = await_partial(head, side, dist + 1, dev, me)
        send_partial(head, side, dist, combine(load_own(head, way * dist, size), got), me, size, dev)

    last_hop = max(ny, nz) // 2
    def keep_arrived(hop):
        for head, size in ((0, ny), (1, nz)):
            for q in ring(hop, size):
                keep_queries(head, q)

    def send_far():
        for head, me, size, dev in rings:
            if size // 2 == last_hop:
                own_part(head, 0, reach(0, size), me, size, dev)

    keep_arrived(0)
    first_round = min(1, last_hop - 1)
    if first_round == 0:
        early(0)
    for hop in range(1, last_hop + 1):
        phase("gather_hop" + str(hop))
        pass_on(hop)
        if hop == min(2, last_hop):
            state_send()
        keep_arrived(hop)
        if hop == first_round:
            phase("early")
            early(hop)
        elif hop > first_round:
            phase("late_queries" + str(hop))
            late_queries(hop)
            if hop == last_hop:
                send_far()
            phase("late_keys" + str(hop))
            late_keys(hop)
            if hop == min(3, last_hop):
                state_prefix()
    phase("partials")
    for dist in (4, 3, 2, 1):
        for head, me, size, dev in rings:
            for side in (1, 0):
                unsent = side == 1 or size // 2 < last_hop
                if dist == reach(side, size) and unsent or dist == 1 and reach(side, size) > 1:
                    own_part(head, side, dist, me, size, dev)
    phase("pass_far")
    for dist in (3, 2):
        if dist == 2:
            state_entry()
            phase("pass_near")
        for head, me, size, dev in rings:
            for side in (1, 0):
                if dist + 1 <= reach(side, size) and dist + 1 > 2:
                    passing(head, side, dist, me, size, dev)
                elif dist == 2 and dist < reach(side, size):
                    own_part(head, side, dist, me, size, dev)

    def finish(head, value):
        top, total, num = value
        att = num[:, :ROWS] / total[:, :ROWS] - lam_ref[head] * num[:, ROWS:] / total[:, ROWS:]
        att = att * lax.rsqrt(jnp.mean(att * att, axis=0, keepdims=True) + EPS)
        lws_ref[head:head + 1, :] = top[:, :ROWS] + jnp.log(total[:, :ROWS])
        return (att.T * attg_ref[...] * 0.8).astype(BF16)

    phase("merge_own")
    att = []
    for head, me, size, dev in rings:
        value = load_own(head, 0, size)
        for dist in (1, 2):
            for side in (1, 0):
                if dist <= reach(side, size):
                    value = combine(value, await_partial(head, side, dist, dev, me))
        att.append(finish(head, value))
    att_rows = jnp.concatenate(att, axis=1)

    phase("rec_result")
    for d in range(1, ny):
        yy = (y + d) % ny
        remote(in_r.at[yy], in_r.at[yy], in_send.at[0], in_recv.at[yy], y_dev(yy)).wait_recv()
    rec = []
    for h in range(2):
        o = ol_scr[h] + dot_nt(qc_scr[h], in_r[:, h].reshape(DV, DV))
        rec.append(norm_rows(o, recg_ref[...]).astype(BF16))
    rec_rows = jnp.concatenate(rec, axis=1)

    phase("project_out")
    for c in wo_copies:
        c.wait()
    width = wo.shape[2] // PARTS
    p_list = []
    for k in range(PARTS):
        cols = slice(k * width, (k + 1) * width)
        part = dot_nn(att_rows, wo[0, :, cols]) + dot_nn(rec_rows, wo[1, :, cols])
        pbuf[k] = part.astype(BF16)
        c = remote(pbuf.at[k], prx.at[k], p_send.at[k], p_recv.at[k], {"tp": t_other})
        c.start()
        p_list.append(c)
    for k in range(PARTS):
        p_list[k].wait_recv()
        out_ref[:, k * width:(k + 1) * width] = (pbuf[k].astype(F32) + prx[k].astype(F32)).astype(BF16)

    phase("drain")
    for c in a_list + r_list + g_list + p_list:
        c.wait_send()
    phase(None)


def hand_over(mixed_ref, log_ref, mixed_out, log_out):
    mixed_out[...] = mixed_ref[...]
    log_out[...] = log_ref[...]


def on_device(nz, ny, tokens, in_gain, wq, wk, wv, wrq, wrf, wri, lam, lb, scale, attg, recg, wa, wr):
    d = tokens.shape[1]
    out_cols = wa.shape[1]
    any_spec = pl.BlockSpec(memory_space=pl.ANY)
    vmem = pl.BlockSpec(memory_space=pltpu.VMEM)
    smem = pl.BlockSpec(memory_space=pltpu.SMEM)
    slice_rows = DV // ny
    st_rows = 2 * slice_rows + 16
    dma = pltpu.SemaphoreType.DMA
    scratch = [
        pltpu.VMEM((ROWS, d), BF16),
        pltpu.VMEM((COLS, d), BF16),
        pltpu.VMEM((2, wa.shape[0], out_cols), BF16),
        pltpu.VMEM((FS, ROWS, d), BF16),
        pltpu.VMEM((FS, ROWS, FIRST), BF16),
        pltpu.VMEM((FS, ROWS, COLS - FIRST), BF16),
        pltpu.VMEM((3, ROWS, FIRST), BF16),
        pltpu.VMEM((3, ROWS, COLS - FIRST), BF16),
        pltpu.VMEM((ny, 3, ROWS, DV), BF16),
        pltpu.VMEM((nz, 3, ROWS, DV), BF16),
        pltpu.VMEM((2, DV, max(ny, nz) * 2 * ROWS), F32),
        pltpu.VMEM((2, 8, max(ny, nz) * 2 * ROWS), F32),
        pltpu.VMEM((2, DV, max(ny, nz) * 2 * ROWS), BF16),
        pltpu.VMEM((2, 2, 5, 2 * DV + 16, ROWS), BF16),
        pltpu.VMEM((2, 2, 5, 2 * DV + 16, ROWS), BF16),
        pltpu.VMEM((ny, st_rows, DV), BF16),
        pltpu.VMEM((ny, st_rows, DV), BF16),
        pltpu.VMEM((st_rows, DV), BF16),
        pltpu.VMEM((nz, st_rows, DV), BF16),
        pltpu.VMEM((ny, 2, slice_rows, DV), BF16),
        pltpu.VMEM((ny, 2, slice_rows, DV), BF16),
        pltpu.VMEM((ny, st_rows, DV), F32),
        pltpu.VMEM((2, ROWS, DV), BF16),
        pltpu.VMEM((2, ROWS, DV), F32),
        pltpu.VMEM((PARTS, ROWS, out_cols // PARTS), BF16),
        pltpu.VMEM((PARTS, ROWS, out_cols // PARTS), BF16),
        dma((9,)), dma((12,)), dma((FS, 4)), dma((3, 2)), dma((FS, 2)),
        dma((2, ny // 2 + 1, 3)), dma((ny, 3)), dma((2, nz // 2 + 1, 3)), dma((nz, 3)),
        dma((2, 2, 5)), dma((2, 2, 5)),
        dma((ny,)), dma((ny,)), dma((nz,)), dma((nz,)), dma((ny,)), dma((ny,)),
        dma((PARTS,)), dma((PARTS,)),
    ]
    mixed, log_sum = pl.pallas_call(
        functools.partial(kernel_body, nz, ny),
        out_shape=(
            jax.ShapeDtypeStruct((ROWS, out_cols), BF16),
            jax.ShapeDtypeStruct((2, ROWS), F32),
        ),
        in_specs=[any_spec, vmem] + [any_spec] * 6 + [smem, vmem, vmem, vmem, vmem, any_spec, any_spec],
        out_specs=(vmem, vmem),
        scratch_shapes=scratch,
        compiler_params=pltpu.CompilerParams(
            collective_id=0, has_side_effects=True, vmem_limit_bytes=56 * 1024 * 1024
        ),
    )(
        tokens, in_gain.reshape(1, d), wq.T, wk.T, wv.T, wrq.T, wrf.T, wri.T, lam, lb,
        scale.reshape(1, ROWS), attg.reshape(1, DV), recg.reshape(1, DV), wa, wr,
    )
    return pl.pallas_call(
        hand_over,
        out_shape=(
            jax.ShapeDtypeStruct((ROWS, out_cols), BF16),
            jax.ShapeDtypeStruct((2, ROWS), F32),
        ),
        in_specs=[vmem, vmem],
        out_specs=(vmem, vmem),
    )(mixed, log_sum)


def plane_of(size):
    nz = 1
    while nz * nz < size:
        nz *= 2
    return nz, size // nz


def solution(mesh):
    nz, ny = plane_of(mesh.shape["sp"])
    col_split = P(None, ("tp", "fs"))
    placed = (
        P(("fs", "sp"), None), P(),
        col_split, col_split, col_split, col_split, col_split, col_split,
        P("tp"), P("tp", None), P(("fs", "sp")), P(), P(),
        P("tp", None), P("tp", None),
    )
    return jax.shard_map(
        functools.partial(on_device, nz, ny),
        mesh=mesh,
        in_specs=placed,
        out_specs=(P(("fs", "sp"), None), P("tp", ("fs", "sp"))),
        check_vma=False,
    )
```

```python
import functools

import jax
import jax.numpy as jnp
from jax import lax
from jax.experimental import pallas as pl
from jax.experimental.pallas import tpu as pltpu
from jax.sharding import PartitionSpec as P

DK = 64
DV = 128
ROWS = 128
COLS = 384
FIRST = 256
EPS = 1e-06
NEG = -1e30
FS = 4
PARTS = 4
MESH = pl.DeviceIdType.MESH
F32 = jnp.float32
BF16 = jnp.bfloat16


def dot_nn(a, b):
    return lax.dot_general(a, b, (((1,), (0,)), ((), ())), preferred_element_type=F32)


def dot_nt(a, b):
    return lax.dot_general(a, b, (((1,), (1,)), ((), ())), preferred_element_type=F32)


def pack_rates(first, second):
    parts = []
    for rate in (first, second):
        high = rate.astype(BF16).astype(F32)
        parts += [jnp.broadcast_to(v, (4, DV)) for v in (high, rate - high)]
    return jnp.concatenate(parts, axis=0).astype(BF16)


def unpack_rates(packed):
    wide = packed.astype(F32)
    return wide[0:1] + wide[4:5], wide[8:9] + wide[12:13]


def pack_stats(rows):
    tile = jnp.zeros((16, DV), F32)
    where = lax.broadcasted_iota(jnp.int32, (16, DV), 0)
    for i, value in enumerate(rows):
        high = value.astype(BF16).astype(F32)
        middle = (value - high).astype(BF16).astype(F32)
        for j, part in enumerate((high, middle, value - high - middle)):
            tile = jnp.where(where == 3 * i + j, part, tile)
    return tile.astype(BF16)


def unpack_stats(packed, count=4):
    wide = packed.astype(F32)
    return [wide[3 * i:3 * i + 1] + wide[3 * i + 1:3 * i + 2] + wide[3 * i + 2:3 * i + 3] for i in range(count)]


def norm_rows(values, gain):
    mean = jnp.mean(values * values, axis=-1, keepdims=True)
    return values * lax.rsqrt(mean + EPS) * gain


def kernel_body(
    nz, ny,
    tok_hbm, gain_ref, wq, wk, wv, wrq, wrf, wri, lam_ref, lb_ref, scale_ref, attg_ref, recg_ref,
    wa_hbm, wr_hbm,
    out_ref, lws_ref,
    tok, wcat, wo, nrm, res, res2, rsend, rsend2,
    gy, gz, acc, stat, qb, po_s, po_r, pf_s, pf_r,
    st_s, st_r, tot_s, tot_r, in_s, in_r, pref, qc_scr, ol_scr,
    pbuf, prx,
    lsem, a_send, a_recv, r_send, r_recv,
    gy_send, gy_recv, gz_send, gz_recv,
    po_send, po_recv, pf_send, pf_recv,
    st_send, st_recv, tot_send, tot_recv, in_send, in_recv,
    p_send, p_recv,
):
    p = lax.axis_index("sp")
    x = lax.axis_index("fs")
    t = lax.axis_index("tp")
    z = p // ny
    y = p % ny
    t_other = 1 - t
    xl = (x + 3) % 4
    xr = (x + 1) % 4
    xo = (x + 2) % 4
    slice_rows = DV // ny

    open_scope = []

    def phase(name):
        if open_scope:
            open_scope.pop().__exit__(None, None, None)
        if name:
            scope = jax.named_scope(name)
            scope.__enter__()
            open_scope.append(scope)

    phase("start")
    weights = (wq, wk, wv, wrq, wrf, wri)
    tok_copy = pltpu.make_async_copy(tok_hbm, tok, lsem.at[0])
    tok_copy.start()
    w_copies = [
        pltpu.make_async_copy(w, wcat.at[pl.ds(i * DK, DK)], lsem.at[1 + i]) for i, w in enumerate(weights)
    ]
    for c in w_copies:
        c.start()
    wo_copies = [
        pltpu.make_async_copy(wa_hbm, wo.at[0], lsem.at[7]),
        pltpu.make_async_copy(wr_hbm, wo.at[1], lsem.at[8]),
    ]
    for c in wo_copies:
        c.start()

    barrier = pltpu.get_barrier_semaphore()

    def greet(dev):
        pl.semaphore_signal(barrier, inc=1, device_id=dev, device_id_type=MESH)

    greet({"tp": t_other})
    for d in range(1, 4):
        greet({"fs": (x + d) % 4})
    for d in range(1, ny):
        greet({"sp": z * ny + (y + d) % ny})
    for d in range(1, nz):
        greet({"sp": ((z + d) % nz) * ny + y})

    def remote(src, dst, ssem, rsem, dev):
        return pltpu.make_async_remote_copy(
            src_ref=src, dst_ref=dst, send_sem=ssem, recv_sem=rsem, device_id=dev, device_id_type=MESH
        )

    def piece(f, tt, pc):
        return nrm.at[f, pl.ds(pl.multiple_of(tt * 64 + pc * 32, 32), 32)]

    def a_sem(f, tt, pc):
        return a_recv.at[f, tt * 2 + pc]

    def normalise(tt, pc):
        rows = pl.ds(pl.multiple_of(tt * 64 + pc * 32, 32), 32)
        nrm[x, rows, :] = norm_rows(tok[rows, :].astype(F32), gain_ref[...]).astype(BF16)

    tok_copy.wait()
    normalise(t, 0)
    normalise(t, 1)
    phase("entry_barrier")
    pl.semaphore_wait(barrier, 1 + 3 + (ny - 1) + (nz - 1))

    def a_start(k, f, pc, dev):
        c = remote(piece(f, t, pc), piece(f, t, pc), a_send.at[0], a_sem(f, t, pc), dev)
        c.start()

    def a_wait(f, tt, pc):
        remote(piece(f, tt, pc), piece(f, tt, pc), a_send.at[0], a_sem(f, tt, pc), {"fs": xr}).wait_recv()

    phase("x_own")
    a_start(0, x, 0, {"fs": xr})
    a_start(1, x, 1, {"fs": xl})
    a_start(2, x, 1, {"fs": xr})
    a_start(3, x, 0, {"fs": xl})
    normalise(t_other, 0)
    normalise(t_other, 1)
    for i in range(6):
        w_copies[i].wait()

    def project(rows):
        return dot_nt(rows, wcat[...]).astype(BF16)

    acc[...] = jnp.zeros_like(acc)
    stat[...] = jnp.full(stat.shape, NEG, F32)
    own = project(nrm[x])
    res[x] = own[:, :FIRST]
    res2[x] = own[:, FIRST:]
    phase("x_forward")
    a_wait(xl, t, 0)
    a_start(4, xl, 0, {"fs": xr})
    a_start(5, xl, 0, {"tp": t_other})
    a_wait(xr, t, 1)
    a_start(6, xr, 1, {"fs": xl})
    a_start(7, xr, 1, {"tp": t_other})
    a_wait(xl, t, 1)
    a_start(8, xl, 1, {"tp": t_other})
    a_wait(xr, t, 0)
    a_start(9, xr, 0, {"tp": t_other})

    def answer(k, f):
        for j, (out, into) in enumerate(((rsend, res), (rsend2, res2))):
            remote(out.at[k], into.at[x], r_send.at[j], r_recv.at[j], {"fs": f}).start()

    phase("x_near")
    for f in (xl, xr):
        a_wait(f, t_other, 0)
        a_wait(f, t_other, 1)
    near = project(jnp.concatenate([nrm[xl], nrm[xr]], axis=0))
    for k in (0, 1):
        rsend[k] = near[k * ROWS:(k + 1) * ROWS, :FIRST]
        rsend2[k] = near[k * ROWS:(k + 1) * ROWS, FIRST:]
    answer(0, xl)
    answer(1, xr)
    phase("x_far")
    a_wait(xo, t, 0)
    a_start(10, xo, 0, {"tp": t_other})
    a_wait(xo, t, 1)
    a_start(11, xo, 1, {"tp": t_other})
    a_wait(xo, t_other, 0)
    a_wait(xo, t_other, 1)
    far = project(nrm[xo])
    rsend[2] = far[:, :FIRST]
    rsend2[2] = far[:, FIRST:]
    answer(2, xo)
    phase("x_answers")
    def all_of(buf, count, send, recv):
        part = buf.at[pl.ds(0, count)]
        return remote(part, part, send, recv, {"tp": t_other})

    all_of(res, 3, r_send.at[0], r_recv.at[0]).wait_recv()

    phase("tiles")
    def tile(kind, h):
        lo, ref = (kind * DK, res) if kind * DK < FIRST else (kind * DK - FIRST, res2)
        return jnp.concatenate([ref[2 * h, :, lo:lo + DK], ref[2 * h + 1, :, lo:lo + DK]], axis=1)

    def value_t(h):
        return tile(2, h).astype(F32).T.astype(BF16)

    scale_q = jnp.asarray(DK ** (-0.5), BF16)
    gy[0, 0] = (tile(0, 0) * scale_q).astype(F32).T.astype(BF16)
    gy[0, 1] = tile(1, 1)
    gy[0, 2] = value_t(1)
    gz[0, 0] = (tile(0, 1) * scale_q).astype(F32).T.astype(BF16)
    gz[0, 1] = tile(1, 0)
    gz[0, 2] = value_t(0)

    def y_dev(yy):
        return {"sp": z * ny + yy}

    def z_dev(zz):
        return {"sp": zz * ny + y}

    def pass_on(hop):
        for k in range(3):
            for buf, sent, got, me, size, dev in (
                (gy, gy_send, gy_recv, y, ny, y_dev), (gz, gz_send, gz_recv, z, nz, z_dev)
            ):
                for way in (1, -1):
                    def carried(h):
                        return 2 * h < size or (2 * h == size and (k % 2 == 0) == (way == 1))

                    here = (-way * hop) % size
                    there = (-way * (hop + 1)) % size
                    dev_next = dev((me + size + way) % size)
                    if hop > 0 and carried(hop):
                        remote(buf.at[here, k], buf.at[here, k], sent.at[0], got.at[here, k], dev_next).wait_recv()
                    if carried(hop + 1):
                        remote(buf.at[here, k], buf.at[there, k], sent.at[0], got.at[there, k], dev_next).start()

    pass_on(0)

    phase("rec_local")
    all_of(res2, 3, r_send.at[1], r_recv.at[1]).wait_recv()
    row = lax.broadcasted_iota(jnp.int32, (ROWS, ROWS), 0)
    col = lax.broadcasted_iota(jnp.int32, (ROWS, ROWS), 1)
    tril = jnp.where(row >= col, 1.0, 0.0).astype(F32)
    rates = []
    scale_col = jnp.broadcast_to(scale_ref[...], (ROWS, ROWS)).T
    for h in range(2):
        rq = tile(3, h).astype(F32)
        rf = tile(4, h).astype(F32)
        ri = tile(5, h)
        edge = lb_ref[h:h + 1, :]
        forget = edge + (1.0 - edge) * jax.nn.sigmoid(rf)
        g = scale_col * jnp.log(forget)
        kk = 1.0 - jnp.exp(g)
        cum = lax.dot_general(
            tril, g, (((1,), (0,)), ((), ())), precision=lax.Precision.HIGHEST, preferred_element_type=F32
        )
        scores = jnp.where(row == col, jnp.sum(rq * kk, axis=-1, keepdims=True), 0.0)
        c8 = cum.reshape(ROWS // 8, 8, DV)
        r8 = lax.broadcasted_iota(jnp.int32, (ROWS // 8, 8, DV), 1)
        for b in (64, 32, 16, 8, 4, 2, 1):
            if b >= 8:
                c3 = cum.reshape(ROWS // (2 * b), 2 * b, DV)
                diff = (c3 - c3[:, b - 1:b, :]).reshape(ROWS, DV)
            else:
                mid = c8[:, b - 1:b, :]
                for first in range(2 * b, 8, 2 * b):
                    mid = jnp.where(r8 >= first, c8[:, first + b - 1:first + b, :], mid)
                diff = (c8 - mid).reshape(ROWS, DV)
            upper = (row & (2 * b - 1)) >= b
            decay = jnp.exp(jnp.where(upper, diff, -diff))
            late = jnp.where(upper, rq * decay, 0.0).astype(BF16)
            early = jnp.where(upper, 0.0, kk * decay).astype(BF16)
            level = dot_nt(late, early)
            scores = scores + jnp.where((row ^ col) < 2 * b, level, 0.0)
        ol_scr[h] = dot_nn(scores.astype(BF16), ri)
        last = cum[ROWS - 1:ROWS, :]
        key_end = (kk * jnp.exp(last - cum)).astype(BF16)
        state_t = dot_nn(ri.astype(F32).T.astype(BF16), key_end)
        qc_scr[h] = (rq * jnp.exp(cum)).astype(BF16)
        st_s[:, h * slice_rows:(h + 1) * slice_rows, :] = state_t.reshape(ny, slice_rows, DV).astype(BF16)
        rates.append(jnp.exp(last))
    packed = pack_rates(*rates)
    for k in range(ny):
        st_s[k, 2 * slice_rows:, :] = packed
    def state_send():
        st_r[y] = st_s[y]
        for d in range(1, ny):
            yy = (y + d) % ny
            remote(st_s.at[yy], st_r.at[y], st_send.at[0], st_recv.at[0], y_dev(yy)).start()

    half = slice_rows

    def step_of(ref):
        d0, d1 = unpack_rates(ref[2 * half:, :])
        return d0, ref[0:half, :].astype(F32), d1, ref[half:2 * half, :].astype(F32)

    def state_prefix():
        phase("rec_prefix")
        all_of(st_r, ny - 1, st_send.at[0], st_recv.at[0]).wait_recv()

        s0 = s1 = jnp.zeros((half, DV), F32)
        c0 = c1 = jnp.ones((1, DV), F32)
        for k in range(ny):
            pref[k, 0:half, :] = s0
            pref[k, half:2 * half, :] = s1
            pref[k, 2 * half:2 * half + 8, :] = jnp.broadcast_to(c0, (8, DV))
            pref[k, 2 * half + 8:2 * half + 16, :] = jnp.broadcast_to(c1, (8, DV))
            d0, a0, d1, a1 = step_of(st_r.at[k])
            s0, s1, c0, c1 = d0 * s0 + a0, d1 * s1 + a1, c0 * d0, c1 * d1
        tot_s[0:half, :] = s0.astype(BF16)
        tot_s[half:2 * half, :] = s1.astype(BF16)
        tot_s[2 * half:, :] = pack_rates(c0, c1)
        for d in range(1, nz):
            zz = (z + d) % nz
            remote(tot_s, tot_r.at[z], tot_send.at[0], tot_recv.at[0], z_dev(zz)).start()

    def state_entry():
        phase("rec_totals")
        all_of(tot_r, nz - 1, tot_send.at[0], tot_recv.at[0]).wait_recv()

        def fold(k, carry):
            d0, a0, d1, a1 = step_of(tot_r.at[k])
            return (d0 * carry[0] + a0, d1 * carry[1] + a1)

        entry = lax.fori_loop(0, z, fold, (jnp.zeros((half, DV), F32), jnp.zeros((half, DV), F32)))
        for k in range(ny):
            for h in range(2):
                d = pref[k, 2 * half + 8 * h:2 * half + 8 * h + 1, :]
                in_s[k, h] = (d * entry[h] + pref[k, h * half:(h + 1) * half, :]).astype(BF16)
        in_r[y] = in_s[y]
        for d in range(1, ny):
            yy = (y + d) % ny
            remote(in_s.at[yy], in_r.at[y], in_send.at[0], in_recv.at[0], y_dev(yy)).start()

    channel = lax.broadcasted_iota(jnp.int32, (ROWS, DV), 0)
    below = (
        lax.broadcasted_iota(jnp.int32, (ROWS, 2 * ROWS), 0)
        <= (lax.broadcasted_iota(jnp.int32, (ROWS, 2 * ROWS), 1) & (ROWS - 1))
    )

    def seen(head, off):
        if off % nz == 0:
            return None
        other = (z + off % nz) % nz
        return other < z if head == 0 else other > z

    def when(condition, body):
        if condition is None:
            body()
        else:
            pl.when(condition)(body)

    def ring(hop, size):
        if hop == 0:
            return [0]
        if 2 * hop < size:
            return [hop, -hop]
        return [hop] if 2 * hop == size else []

    def within(hop, size):
        return [o for h in range(hop + 1) for o in ring(h, size)]

    def arrival(off, size):
        return [o % size for o in within(size, size)].index(off % size)

    def sides(head):
        return (gy, gz, ny, nz) if head == 0 else (gz, gy, nz, ny)

    def keep_queries(head, off):
        q_buf, _, q_size, _ = sides(head)
        queries = q_buf[off % q_size, 0]
        zero = jnp.zeros_like(queries)
        at = arrival(off, q_size) * 2 * ROWS
        qb[head, :, at:at + ROWS] = jnp.where(channel < DK, queries, zero)
        qb[head, :, at + ROWS:at + 2 * ROWS] = jnp.where(channel < DK, zero, queries)

    def hidden(head, q_off, k_off):
        _, _, q_size, k_size = sides(head)
        if head == 0:
            if k_off % nz == 0:
                return y > (y + q_off % ny) % ny
            return (z + k_off % nz) % nz > z
        if q_off % nz == 0:
            return (y + k_off % ny) % ny > y
        return (z + q_off % nz) % nz < z

    def attend(head, q_offs, k_offs, checked=True):
        _, kv_buf, q_size, k_size = sides(head)
        if not q_offs or not k_offs:
            return
        lo = arrival(q_offs[0], q_size) * 2 * ROWS
        hi = lo + len(q_offs) * 2 * ROWS
        slots = [o % k_size for o in k_offs]
        s = dot_nn(jnp.concatenate([kv_buf[i, 1] for i in slots], axis=0), qb[head, :, lo:hi])
        parts = []
        for i, k_off in enumerate(k_offs):
            part = s[i * ROWS:(i + 1) * ROWS]
            blocks = []
            for j, q_off in enumerate(q_offs):
                block = part[:, j * 2 * ROWS:(j + 1) * 2 * ROWS]
                if q_off % q_size == 0 and k_off % k_size == 0:
                    block = jnp.where(below, block, NEG)
                elif checked or (k_off if head == 0 else q_off) % nz == 0:
                    block = block + jnp.where(hidden(head, q_off, k_off), NEG, 0.0).astype(F32)
                blocks.append(block)
            parts.append(jnp.concatenate(blocks, axis=1))
        width = hi - lo
        best = jnp.max(functools.reduce(jnp.maximum, parts).reshape(ROWS // 8, 8, width), axis=0)
        top = stat[head, 0:1, lo:hi]
        now = jnp.maximum(top, jnp.max(best, axis=0, keepdims=True))
        es = [jnp.exp(part - now) for part in parts]
        summed = functools.reduce(jnp.add, [jnp.sum(e.reshape(ROWS // 8, 8, width), axis=0) for e in es])
        new = dot_nn(
            jnp.concatenate([kv_buf[i, 2] for i in slots], axis=1),
            jnp.concatenate([e.astype(BF16) for e in es], axis=0),
        )
        keep = jnp.exp(top - now)
        stat[head, 0:1, lo:hi] = now
        stat[head, 1:2, lo:hi] = keep * stat[head, 1:2, lo:hi] + jnp.sum(summed, axis=0, keepdims=True)
        acc[head, :, lo:hi] = keep * acc[head, :, lo:hi] + new

    def early(hop):
        queries, keys = within(hop, ny), within(hop, nz)
        for k in keys:
            when(seen(0, k), lambda k=k: attend(0, queries, [k], False))
        queries, keys = within(hop, nz), within(hop, ny)
        for q in queries:
            when(seen(1, q), lambda q=q: attend(1, [q], keys, False))

    def late_queries(hop):
        keys = within(hop, nz)
        attend(0, ring(hop, ny), [k for k in keys if k <= 0])
        rest = [k for k in keys if k > 0]
        if rest and ring(hop, ny):
            pl.when(z + max(rest) >= nz)(lambda: attend(0, ring(hop, ny), rest))
        for q in ring(hop, nz):
            when(seen(1, q), lambda q=q: attend(1, [q], within(hop, ny), False))

    def late_keys(hop):
        for k in ring(hop, nz):
            when(seen(0, k), lambda k=k: attend(0, within(hop - 1, ny), [k], False))
        attend(1, within(hop - 1, nz), ring(hop, ny))

    rings = ((0, y, ny, y_dev), (1, z, nz, z_dev))

    def reach(side, size):
        return (size - 1) // 2 if side == 1 or size == 8 else size // 2

    routes = [
        (head, side, dist) for head, _, size, _ in rings for side in (0, 1) for dist in range(1, reach(side, size) + 1)
    ]
    halves = [(head, side) for head, _, size, _ in rings if size == 8 for side in (0, 1)]

    def send_half(head, side, me, size, dev):
        top, total, num = load_own(head, size // 2, size)
        lanes = slice(side * ROWS, (side + 1) * ROWS)
        at = halves.index((head, side))
        pf_s[at, 0:DV, :] = num[:, lanes].astype(BF16)
        pf_s[at, DV:, :] = pack_stats([top[:, lanes], total[:, lanes]])
        hop = -2 if side == 0 else 2
        remote(pf_s.at[at], pf_r.at[at], pf_send.at[0], pf_recv.at[at], dev((me + size + hop) % size)).start()

    def combine_half(value, head, side, dev, me):
        at = halves.index((head, side))
        remote(pf_r.at[at], pf_r.at[at], pf_send.at[0], pf_recv.at[at], dev(me)).wait_recv()
        lanes = slice(side * ROWS, (side + 1) * ROWS)
        new_top, new_total = unpack_stats(pf_r[at, DV:, :], 2)
        top, total, num = (v[:, lanes] for v in value)
        now = jnp.maximum(top, new_top)
        keep, weight = jnp.exp(top - now), jnp.exp(new_top - now)
        merged = (now, keep * total + weight * new_total, keep * num + weight * pf_r[at, 0:DV, :].astype(F32))
        rest = [v[:, (1 - side) * ROWS:(2 - side) * ROWS] for v in value]
        pairs = zip(merged, rest) if side == 0 else zip(rest, merged)
        return tuple(jnp.concatenate(pair, axis=1) for pair in pairs)

    def load_own(head, off, size):
        lo = arrival(off, size) * 2 * ROWS
        hi = lo + 2 * ROWS
        return stat[head, 0:1, lo:hi], stat[head, 1:2, lo:hi], acc[head, :, lo:hi]

    def combine(one, message):
        top, total, num = one
        t0, l0, t1, l1 = unpack_stats(message[2 * DV:, :])
        new_top = jnp.concatenate([t0, t1], axis=1)
        now = jnp.maximum(top, new_top)
        keep = jnp.exp(top - now)
        weight = jnp.exp(new_top - now)
        new_num = jnp.concatenate([message[0:DV, :].astype(F32), message[DV:2 * DV, :].astype(F32)], axis=1)
        total = keep * total + weight * jnp.concatenate([l0, l1], axis=1)
        return now, total, keep * num + weight * new_num

    def send_partial(head, side, dist, value, me, size, dev):
        way = -1 if side == 0 else 1
        top, total, num = value
        at = routes.index((head, side, dist))
        out = po_s.at[at]
        out[0:DV, :] = num[:, :ROWS].astype(BF16)
        out[DV:2 * DV, :] = num[:, ROWS:].astype(BF16)
        out[2 * DV:, :] = pack_stats([top[:, :ROWS], total[:, :ROWS], top[:, ROWS:], total[:, ROWS:]])
        step = min(dist, 2) if dist < 3 else 1
        remote(
            out, po_r.at[at], po_send.at[0], po_recv.at[at], dev((me + size + way * step) % size)
        ).start()

    def await_partial(head, side, dist, dev, me):
        at = routes.index((head, side, dist))
        remote(po_r.at[at], po_r.at[at], po_send.at[0], po_recv.at[at], dev(me)).wait_recv()
        return po_r.at[at]


    def own_part(head, side, dist, me, size, dev):
        way = -1 if side == 0 else 1
        send_partial(head, side, dist, load_own(head, way * dist, size), me, size, dev)

    def passing(head, side, dist, me, size, dev):
        way = -1 if side == 0 else 1
        value = load_own(head, way * dist, size)
        if size == 8:
            value = combine_half(value, head, side, dev, me)
        for farther in range(dist + 1, reach(side, size) + 1):
            value = combine(value, await_partial(head, side, farther, dev, me))
        send_partial(head, side, dist, value, me, size, dev)

    last_hop = max(ny, nz) // 2
    def keep_arrived(hop):
        for head, size in ((0, ny), (1, nz)):
            for q in ring(hop, size):
                keep_queries(head, q)

    def send_far():
        for head, me, size, dev in rings:
            if size == 8:
                for side in (0, 1):
                    send_half(head, side, me, size, dev)
            elif size // 2 == last_hop:
                own_part(head, 0, reach(0, size), me, size, dev)

    keep_arrived(0)
    first_round = min(1, last_hop - 1)
    if first_round == 0:
        early(0)
    for hop in range(1, last_hop + 1):
        phase("gather_hop" + str(hop))
        pass_on(hop)
        if hop == min(2, last_hop):
            state_send()
        keep_arrived(hop)
        if hop == first_round:
            phase("early")
            early(hop)
        elif hop > first_round:
            phase("late_queries" + str(hop))
            late_queries(hop)
            if hop == last_hop:
                send_far()
            phase("late_keys" + str(hop))
            late_keys(hop)
            if hop == min(3, last_hop):
                state_prefix()
    phase("partials")
    for dist in (3, 1):
        for head, me, size, dev in rings:
            for side in (1, 0):
                unsent = side == 1 or size // 2 < last_hop or size == 8
                if dist == reach(side, size) and unsent or dist == 1 and reach(side, size) > 1:
                    own_part(head, side, dist, me, size, dev)
    phase("pass_far")
    for side in (1, 0):
        for head, me, size, dev in rings:
            if reach(side, size) > 2:
                passing(head, side, 2, me, size, dev)
            elif reach(side, size) == 2 and size // 2 < last_hop:
                own_part(head, side, 2, me, size, dev)
        if side == 1:
            state_entry()
            phase("pass_near")

    def finish(head, value):
        top, total, num = value
        att = num[:, :ROWS] / total[:, :ROWS] - lam_ref[head] * num[:, ROWS:] / total[:, ROWS:]
        att = att * lax.rsqrt(jnp.mean(att * att, axis=0, keepdims=True) + EPS)
        lws_ref[head:head + 1, :] = top[:, :ROWS] + jnp.log(total[:, :ROWS])
        return (att.T * attg_ref[...] * 0.8).astype(BF16)

    phase("merge_own")
    att = []
    for head, me, size, dev in rings:
        value = load_own(head, 0, size)
        for dist in (1, 2):
            for side in (1, 0):
                if dist <= reach(side, size):
                    value = combine(value, await_partial(head, side, dist, dev, me))
        att.append(finish(head, value))
    att_rows = jnp.concatenate(att, axis=1)

    phase("rec_result")
    all_of(in_r, ny - 1, in_send.at[0], in_recv.at[0]).wait_recv()
    rec = []
    for h in range(2):
        o = ol_scr[h] + dot_nt(qc_scr[h], in_r[:, h].reshape(DV, DV))
        rec.append(norm_rows(o, recg_ref[...]).astype(BF16))
    rec_rows = jnp.concatenate(rec, axis=1)

    phase("project_out")
    for c in wo_copies:
        c.wait()
    width = wo.shape[2] // PARTS
    p_list = []
    for k in range(PARTS):
        cols = slice(k * width, (k + 1) * width)
        part = dot_nn(att_rows, wo[0, :, cols]) + dot_nn(rec_rows, wo[1, :, cols])
        pbuf[k] = part.astype(BF16)
        c = remote(pbuf.at[k], prx.at[k], p_send.at[0], p_recv.at[k], {"tp": t_other})
        c.start()
        p_list.append(c)
    for k in range(PARTS):
        p_list[k].wait_recv()
        out_ref[:, k * width:(k + 1) * width] = (pbuf[k].astype(F32) + prx[k].astype(F32)).astype(BF16)

    phase("drain")
    for buf, count, sem in (
        (nrm, 3, a_send.at[0]), (rsend, 3, r_send.at[0]), (rsend2, 3, r_send.at[1]),
        (gy, ny - 1, gy_send.at[0]), (gz, nz - 1, gz_send.at[0]), (st_r, ny - 1, st_send.at[0]),
        (tot_r, nz - 1, tot_send.at[0]), (in_r, ny - 1, in_send.at[0]), (po_s, len(routes), po_send.at[0]),
        (pf_s, len(halves), pf_send.at[0]), (pbuf, PARTS, p_send.at[0]),
    ):
        if count:
            all_of(buf, count, sem, sem).wait_send()
    phase(None)


def on_device(nz, ny, tokens, in_gain, wq, wk, wv, wrq, wrf, wri, lam, lb, scale, attg, recg, wa, wr):
    d = tokens.shape[1]
    out_cols = wa.shape[1]
    any_spec = pl.BlockSpec(memory_space=pl.ANY)
    vmem = pl.BlockSpec(memory_space=pltpu.VMEM)
    smem = pl.BlockSpec(memory_space=pltpu.SMEM)
    slice_rows = DV // ny
    st_rows = 2 * slice_rows + 16
    dma = pltpu.SemaphoreType.DMA
    scratch = [
        pltpu.VMEM((ROWS, d), BF16),
        pltpu.VMEM((COLS, d), BF16),
        pltpu.VMEM((2, wa.shape[0], out_cols), BF16),
        pltpu.VMEM((FS, ROWS, d), BF16),
        pltpu.VMEM((FS, ROWS, FIRST), BF16),
        pltpu.VMEM((FS, ROWS, COLS - FIRST), BF16),
        pltpu.VMEM((3, ROWS, FIRST), BF16),
        pltpu.VMEM((3, ROWS, COLS - FIRST), BF16),
        pltpu.VMEM((ny, 3, ROWS, DV), BF16),
        pltpu.VMEM((nz, 3, ROWS, DV), BF16),
        pltpu.VMEM((2, DV, max(ny, nz) * 2 * ROWS), F32),
        pltpu.VMEM((2, 8, max(ny, nz) * 2 * ROWS), F32),
        pltpu.VMEM((2, DV, max(ny, nz) * 2 * ROWS), BF16),
        pltpu.VMEM((12, 2 * DV + 16, ROWS), BF16),
        pltpu.VMEM((12, 2 * DV + 16, ROWS), BF16),
        pltpu.VMEM((4, DV + 16, ROWS), BF16),
        pltpu.VMEM((4, DV + 16, ROWS), BF16),
        pltpu.VMEM((ny, st_rows, DV), BF16),
        pltpu.VMEM((ny, st_rows, DV), BF16),
        pltpu.VMEM((st_rows, DV), BF16),
        pltpu.VMEM((nz, st_rows, DV), BF16),
        pltpu.VMEM((ny, 2, slice_rows, DV), BF16),
        pltpu.VMEM((ny, 2, slice_rows, DV), BF16),
        pltpu.VMEM((ny, st_rows, DV), F32),
        pltpu.VMEM((2, ROWS, DV), BF16),
        pltpu.VMEM((2, ROWS, DV), F32),
        pltpu.VMEM((PARTS, ROWS, out_cols // PARTS), BF16),
        pltpu.VMEM((PARTS, ROWS, out_cols // PARTS), BF16),
        dma((9,)), dma((1,)), dma((FS, 4)), dma((2,)), dma((2,)),
        dma((1,)), dma((ny, 3)), dma((1,)), dma((nz, 3)),
        dma((1,)), dma((12,)), dma((1,)), dma((4,)),
        dma((1,)), dma((1,)), dma((1,)), dma((1,)), dma((1,)), dma((1,)),
        dma((1,)), dma((PARTS,)),
    ]
    mixed, log_sum = pl.pallas_call(
        functools.partial(kernel_body, nz, ny),
        out_shape=(pltpu.VMEM((ROWS, out_cols), BF16), pltpu.VMEM((2, ROWS), F32)),
        in_specs=[any_spec, vmem] + [any_spec] * 6 + [smem, vmem, vmem, vmem, vmem, any_spec, any_spec],
        out_specs=(vmem, vmem),
        scratch_shapes=scratch,
        compiler_params=pltpu.CompilerParams(
            collective_id=0, has_side_effects=True, vmem_limit_bytes=56 * 1024 * 1024
        ),
    )(
        tokens, in_gain.reshape(1, d), wq.T, wk.T, wv.T, wrq.T, wrf.T, wri.T, lam, lb,
        scale.reshape(1, ROWS), attg.reshape(1, DV), recg.reshape(1, DV), wa, wr,
    )
    return mixed, log_sum


def plane_of(size):
    nz = 1
    while nz * nz < size:
        nz *= 2
    return nz, size // nz


def solution(mesh):
    nz, ny = plane_of(mesh.shape["sp"])
    col_split = P(None, ("tp", "fs"))
    placed = (
        P(("fs", "sp"), None), P(),
        col_split, col_split, col_split, col_split, col_split, col_split,
        P("tp"), P("tp", None), P(("fs", "sp")), P(), P(),
        P("tp", None), P("tp", None),
    )
    return jax.shard_map(
        functools.partial(on_device, nz, ny),
        mesh=mesh,
        in_specs=placed,
        out_specs=(P(("fs", "sp"), None), P("tp", ("fs", "sp"))),
        check_vma=False,
    )
```

```python
import functools

import jax
import jax.numpy as jnp
from jax import lax
from jax.experimental import pallas as pl
from jax.experimental.pallas import tpu as pltpu
from jax.sharding import PartitionSpec as P

DK = 64
DV = 128
ROWS = 128
COLS = 384
FIRST = 256
EPS = 1e-06
NEG = -1e30
FS = 4
PARTS = 4
MESH = pl.DeviceIdType.MESH
F32 = jnp.float32
BF16 = jnp.bfloat16


def dot_nn(a, b):
    return lax.dot_general(a, b, (((1,), (0,)), ((), ())), preferred_element_type=F32)


def dot_nt(a, b):
    return lax.dot_general(a, b, (((1,), (1,)), ((), ())), preferred_element_type=F32)


def pack_rates(first, second):
    parts = []
    for rate in (first, second):
        high = rate.astype(BF16).astype(F32)
        parts += [jnp.broadcast_to(v, (4, DV)) for v in (high, rate - high)]
    return jnp.concatenate(parts, axis=0).astype(BF16)


def unpack_rates(packed):
    wide = packed.astype(F32)
    return wide[0:1] + wide[4:5], wide[8:9] + wide[12:13]


def pack_stats(rows):
    tile = jnp.zeros((16, DV), F32)
    where = lax.broadcasted_iota(jnp.int32, (16, DV), 0)
    for i, value in enumerate(rows):
        high = value.astype(BF16).astype(F32)
        middle = (value - high).astype(BF16).astype(F32)
        for j, part in enumerate((high, middle, value - high - middle)):
            tile = jnp.where(where == 3 * i + j, part, tile)
    return tile.astype(BF16)


def unpack_stats(packed, count=4):
    wide = packed.astype(F32)
    return [wide[3 * i:3 * i + 1] + wide[3 * i + 1:3 * i + 2] + wide[3 * i + 2:3 * i + 3] for i in range(count)]


def norm_rows(values, gain):
    mean = jnp.mean(values * values, axis=-1, keepdims=True)
    return values * lax.rsqrt(mean + EPS) * gain


def kernel_body(
    nz, ny,
    tok_hbm, gain_ref, wq, wk, wv, wrq, wrf, wri, lam_ref, lb_ref, scale_ref, attg_ref, recg_ref,
    wa_hbm, wr_hbm,
    out_ref, lws_ref,
    tok, wcat, wo, nrm, res, res2, rsend, rsend2,
    gy, gz, acc, stat, qb, po_s, po_r, pf_s, pf_r,
    st_s, st_r, tot_s, tot_r, in_s, in_r, pref, qc_scr, ol_scr,
    pbuf, prx, half_out,
    lsem, a_send, a_recv, r_send, r_recv,
    gy_send, gy_recv, gz_send, gz_recv,
    po_send, po_recv, pf_send, pf_recv,
    st_send, st_recv, tot_send, tot_recv, in_send, in_recv,
    p_send, p_recv,
):
    p = lax.axis_index("sp")
    x = lax.axis_index("fs")
    t = lax.axis_index("tp")
    z = p // ny
    y = p % ny
    t_other = 1 - t
    xl = (x + 3) % 4
    xr = (x + 1) % 4
    xo = (x + 2) % 4
    slice_rows = DV // ny

    open_scope = []

    def phase(name):
        if open_scope:
            open_scope.pop().__exit__(None, None, None)
        if name:
            scope = jax.named_scope(name)
            scope.__enter__()
            open_scope.append(scope)

    phase("start")
    weights = (wq, wk, wv, wrq, wrf, wri)
    tok_copy = pltpu.make_async_copy(tok_hbm, tok, lsem.at[0])
    tok_copy.start()
    w_copies = [
        pltpu.make_async_copy(w, wcat.at[pl.ds(i * DK, DK)], lsem.at[1 + i]) for i, w in enumerate(weights)
    ]
    for c in w_copies:
        c.start()
    wo_copies = [
        pltpu.make_async_copy(wa_hbm, wo.at[0], lsem.at[7]),
        pltpu.make_async_copy(wr_hbm, wo.at[1], lsem.at[8]),
    ]
    for c in wo_copies:
        c.start()

    barrier = pltpu.get_barrier_semaphore()

    def greet(dev):
        pl.semaphore_signal(barrier, inc=1, device_id=dev, device_id_type=MESH)

    greet({"tp": t_other})
    for d in range(1, 4):
        greet({"fs": (x + d) % 4})
    for d in range(1, ny):
        greet({"sp": z * ny + (y + d) % ny})
    for d in range(1, nz):
        greet({"sp": ((z + d) % nz) * ny + y})

    def remote(src, dst, ssem, rsem, dev):
        return pltpu.make_async_remote_copy(
            src_ref=src, dst_ref=dst, send_sem=ssem, recv_sem=rsem, device_id=dev, device_id_type=MESH
        )

    def piece(f, tt, pc):
        return nrm.at[f, pl.ds(pl.multiple_of(tt * 64 + pc * 32, 32), 32)]

    def a_sem(f, tt, pc):
        return a_recv.at[f, tt * 2 + pc]

    def normalise(tt, pc):
        rows = pl.ds(pl.multiple_of(tt * 64 + pc * 32, 32), 32)
        nrm[x, rows, :] = norm_rows(tok[rows, :].astype(F32), gain_ref[...]).astype(BF16)

    tok_copy.wait()
    normalise(t, 0)
    normalise(t, 1)
    phase("entry_barrier")
    pl.semaphore_wait(barrier, 1 + 3 + (ny - 1) + (nz - 1))

    def a_start(k, f, pc, dev):
        c = remote(piece(f, t, pc), piece(f, t, pc), a_send.at[0], a_sem(f, t, pc), dev)
        c.start()

    def a_wait(f, tt, pc):
        remote(piece(f, tt, pc), piece(f, tt, pc), a_send.at[0], a_sem(f, tt, pc), {"fs": xr}).wait_recv()

    phase("x_own")
    a_start(0, x, 0, {"fs": xr})
    a_start(1, x, 1, {"fs": xl})
    a_start(2, x, 1, {"fs": xr})
    a_start(3, x, 0, {"fs": xl})
    normalise(t_other, 0)
    normalise(t_other, 1)
    for i in range(6):
        w_copies[i].wait()

    def project(rows):
        return dot_nt(rows, wcat[...]).astype(BF16)

    acc[...] = jnp.zeros_like(acc)
    stat[...] = jnp.full(stat.shape, NEG, F32)
    own = project(nrm[x])
    res[x] = own[:, :FIRST]
    res2[x] = own[:, FIRST:]
    phase("x_forward")
    a_wait(xl, t, 0)
    a_start(4, xl, 0, {"fs": xr})
    a_start(5, xl, 0, {"tp": t_other})
    a_wait(xr, t, 1)
    a_start(6, xr, 1, {"fs": xl})
    a_start(7, xr, 1, {"tp": t_other})
    a_wait(xl, t, 1)
    a_start(8, xl, 1, {"tp": t_other})
    a_wait(xr, t, 0)
    a_start(9, xr, 0, {"tp": t_other})

    def answer(k, f):
        for j, (out, into) in enumerate(((rsend, res), (rsend2, res2))):
            remote(out.at[k], into.at[x], r_send.at[j], r_recv.at[j], {"fs": f}).start()

    phase("x_near")
    for f in (xl, xr):
        a_wait(f, t_other, 0)
        a_wait(f, t_other, 1)
    near = project(jnp.concatenate([nrm[xl], nrm[xr]], axis=0))
    for k in (0, 1):
        rsend[k] = near[k * ROWS:(k + 1) * ROWS, :FIRST]
        rsend2[k] = near[k * ROWS:(k + 1) * ROWS, FIRST:]
    answer(0, xl)
    answer(1, xr)
    phase("x_far")
    a_wait(xo, t, 0)
    a_start(10, xo, 0, {"tp": t_other})
    a_wait(xo, t, 1)
    a_start(11, xo, 1, {"tp": t_other})
    a_wait(xo, t_other, 0)
    a_wait(xo, t_other, 1)
    far = project(nrm[xo])
    rsend[2] = far[:, :FIRST]
    rsend2[2] = far[:, FIRST:]
    answer(2, xo)
    phase("x_answers")
    def all_of(buf, count, send, recv):
        part = buf.at[pl.ds(0, count)]
        return remote(part, part, send, recv, {"tp": t_other})

    all_of(res, 3, r_send.at[0], r_recv.at[0]).wait_recv()

    phase("tiles")
    def tile(kind, h):
        lo, ref = (kind * DK, res) if kind * DK < FIRST else (kind * DK - FIRST, res2)
        return jnp.concatenate([ref[2 * h, :, lo:lo + DK], ref[2 * h + 1, :, lo:lo + DK]], axis=1)

    def value_t(h):
        return tile(2, h).astype(F32).T.astype(BF16)

    scale_q = jnp.asarray(DK ** (-0.5), BF16)
    gy[0, 0] = (tile(0, 0) * scale_q).astype(F32).T.astype(BF16)
    gy[0, 1] = tile(1, 1)
    gy[0, 2] = value_t(1)
    gz[0, 0] = (tile(0, 1) * scale_q).astype(F32).T.astype(BF16)
    gz[0, 1] = tile(1, 0)
    gz[0, 2] = value_t(0)

    def y_dev(yy):
        return {"sp": z * ny + yy}

    def z_dev(zz):
        return {"sp": zz * ny + y}

    def pass_on(hop):
        for k in range(3):
            for buf, sent, got, me, size, dev in (
                (gy, gy_send, gy_recv, y, ny, y_dev), (gz, gz_send, gz_recv, z, nz, z_dev)
            ):
                for way in (1, -1):
                    def carried(h):
                        return 2 * h < size or (2 * h == size and (k % 2 == 0) == (way == 1))

                    here = (-way * hop) % size
                    there = (-way * (hop + 1)) % size
                    dev_next = dev((me + size + way) % size)
                    if hop > 0 and carried(hop):
                        remote(buf.at[here, k], buf.at[here, k], sent.at[0], got.at[here, k], dev_next).wait_recv()
                    if carried(hop + 1):
                        remote(buf.at[here, k], buf.at[there, k], sent.at[0], got.at[there, k], dev_next).start()

    pass_on(0)

    phase("rec_local")
    all_of(res2, 3, r_send.at[1], r_recv.at[1]).wait_recv()
    row = lax.broadcasted_iota(jnp.int32, (ROWS, ROWS), 0)
    col = lax.broadcasted_iota(jnp.int32, (ROWS, ROWS), 1)
    tril = jnp.where(row >= col, 1.0, 0.0).astype(F32)
    rates = []
    scale_col = jnp.broadcast_to(scale_ref[...], (ROWS, ROWS)).T
    for h in range(2):
        rq = tile(3, h).astype(F32)
        rf = tile(4, h).astype(F32)
        ri = tile(5, h)
        edge = lb_ref[h:h + 1, :]
        forget = edge + (1.0 - edge) * jax.nn.sigmoid(rf)
        g = scale_col * jnp.log(forget)
        kk = 1.0 - jnp.exp(g)
        cum = lax.dot_general(
            tril, g, (((1,), (0,)), ((), ())), precision=lax.Precision.HIGHEST, preferred_element_type=F32
        )
        scores = jnp.where(row == col, jnp.sum(rq * kk, axis=-1, keepdims=True), 0.0)
        c8 = cum.reshape(ROWS // 8, 8, DV)
        r8 = lax.broadcasted_iota(jnp.int32, (ROWS // 8, 8, DV), 1)
        for b in (64, 32, 16, 8, 4, 2, 1):
            if b >= 8:
                c3 = cum.reshape(ROWS // (2 * b), 2 * b, DV)
                diff = (c3 - c3[:, b - 1:b, :]).reshape(ROWS, DV)
            else:
                mid = c8[:, b - 1:b, :]
                for first in range(2 * b, 8, 2 * b):
                    mid = jnp.where(r8 >= first, c8[:, first + b - 1:first + b, :], mid)
                diff = (c8 - mid).reshape(ROWS, DV)
            upper = (row & (2 * b - 1)) >= b
            decay = jnp.exp(jnp.where(upper, diff, -diff))
            late = jnp.where(upper, rq * decay, 0.0).astype(BF16)
            early = jnp.where(upper, 0.0, kk * decay).astype(BF16)
            level = dot_nt(late, early)
            scores = scores + jnp.where((row ^ col) < 2 * b, level, 0.0)
        ol_scr[h] = dot_nn(scores.astype(BF16), ri)
        last = cum[ROWS - 1:ROWS, :]
        key_end = (kk * jnp.exp(last - cum)).astype(BF16)
        state_t = dot_nn(ri.astype(F32).T.astype(BF16), key_end)
        qc_scr[h] = (rq * jnp.exp(cum)).astype(BF16)
        st_s[:, h * slice_rows:(h + 1) * slice_rows, :] = state_t.reshape(ny, slice_rows, DV).astype(BF16)
        rates.append(jnp.exp(last))
    packed = pack_rates(*rates)
    for k in range(ny):
        st_s[k, 2 * slice_rows:, :] = packed
    def state_send():
        st_r[y] = st_s[y]
        for d in range(1, ny):
            yy = (y + d) % ny
            remote(st_s.at[yy], st_r.at[y], st_send.at[0], st_recv.at[0], y_dev(yy)).start()

    half = slice_rows

    def step_of(ref):
        d0, d1 = unpack_rates(ref[2 * half:, :])
        return d0, ref[0:half, :].astype(F32), d1, ref[half:2 * half, :].astype(F32)

    def state_prefix():
        phase("rec_prefix")
        all_of(st_r, ny - 1, st_send.at[0], st_recv.at[0]).wait_recv()

        s0 = s1 = jnp.zeros((half, DV), F32)
        c0 = c1 = jnp.ones((1, DV), F32)
        for k in range(ny):
            pref[k, 0:half, :] = s0
            pref[k, half:2 * half, :] = s1
            pref[k, 2 * half:2 * half + 8, :] = jnp.broadcast_to(c0, (8, DV))
            pref[k, 2 * half + 8:2 * half + 16, :] = jnp.broadcast_to(c1, (8, DV))
            d0, a0, d1, a1 = step_of(st_r.at[k])
            s0, s1, c0, c1 = d0 * s0 + a0, d1 * s1 + a1, c0 * d0, c1 * d1
        tot_s[0:half, :] = s0.astype(BF16)
        tot_s[half:2 * half, :] = s1.astype(BF16)
        tot_s[2 * half:, :] = pack_rates(c0, c1)
        for d in range(1, nz):
            zz = (z + d) % nz
            remote(tot_s, tot_r.at[z], tot_send.at[0], tot_recv.at[0], z_dev(zz)).start()

    def state_entry():
        phase("rec_totals")
        all_of(tot_r, nz - 1, tot_send.at[0], tot_recv.at[0]).wait_recv()

        def fold(k, carry):
            d0, a0, d1, a1 = step_of(tot_r.at[k])
            return (d0 * carry[0] + a0, d1 * carry[1] + a1)

        entry = lax.fori_loop(0, z, fold, (jnp.zeros((half, DV), F32), jnp.zeros((half, DV), F32)))
        for k in range(ny):
            for h in range(2):
                d = pref[k, 2 * half + 8 * h:2 * half + 8 * h + 1, :]
                in_s[k, h] = (d * entry[h] + pref[k, h * half:(h + 1) * half, :]).astype(BF16)
        in_r[y] = in_s[y]
        for d in range(1, ny):
            yy = (y + d) % ny
            remote(in_s.at[yy], in_r.at[y], in_send.at[0], in_recv.at[0], y_dev(yy)).start()

    channel = lax.broadcasted_iota(jnp.int32, (ROWS, DV), 0)
    below = (
        lax.broadcasted_iota(jnp.int32, (ROWS, 2 * ROWS), 0)
        <= (lax.broadcasted_iota(jnp.int32, (ROWS, 2 * ROWS), 1) & (ROWS - 1))
    )

    def seen(head, off):
        if off % nz == 0:
            return None
        other = (z + off % nz) % nz
        return other < z if head == 0 else other > z

    def when(condition, body):
        if condition is None:
            body()
        else:
            pl.when(condition)(body)

    def ring(hop, size):
        if hop == 0:
            return [0]
        if 2 * hop < size:
            return [hop, -hop]
        return [hop] if 2 * hop == size else []

    def within(hop, size):
        return [o for h in range(hop + 1) for o in ring(h, size)]

    def arrival(off, size):
        return [o % size for o in within(size, size)].index(off % size)

    def sides(head):
        return (gy, gz, ny, nz) if head == 0 else (gz, gy, nz, ny)

    def keep_queries(head, off):
        q_buf, _, q_size, _ = sides(head)
        queries = q_buf[off % q_size, 0]
        zero = jnp.zeros_like(queries)
        at = arrival(off, q_size) * 2 * ROWS
        qb[head, :, at:at + ROWS] = jnp.where(channel < DK, queries, zero)
        qb[head, :, at + ROWS:at + 2 * ROWS] = jnp.where(channel < DK, zero, queries)

    def hidden(head, q_off, k_off):
        _, _, q_size, k_size = sides(head)
        if head == 0:
            if k_off % nz == 0:
                return y > (y + q_off % ny) % ny
            return (z + k_off % nz) % nz > z
        if q_off % nz == 0:
            return (y + k_off % ny) % ny > y
        return (z + q_off % nz) % nz < z

    def attend(head, q_offs, k_offs, checked=True):
        _, kv_buf, q_size, k_size = sides(head)
        if not q_offs or not k_offs:
            return
        lo = arrival(q_offs[0], q_size) * 2 * ROWS
        hi = lo + len(q_offs) * 2 * ROWS
        slots = [o % k_size for o in k_offs]
        s = dot_nn(jnp.concatenate([kv_buf[i, 1] for i in slots], axis=0), qb[head, :, lo:hi])
        parts = []
        for i, k_off in enumerate(k_offs):
            part = s[i * ROWS:(i + 1) * ROWS]
            blocks = []
            for j, q_off in enumerate(q_offs):
                block = part[:, j * 2 * ROWS:(j + 1) * 2 * ROWS]
                if q_off % q_size == 0 and k_off % k_size == 0:
                    block = jnp.where(below, block, NEG)
                elif checked or (k_off if head == 0 else q_off) % nz == 0:
                    block = block + jnp.where(hidden(head, q_off, k_off), NEG, 0.0).astype(F32)
                blocks.append(block)
            parts.append(jnp.concatenate(blocks, axis=1))
        width = hi - lo
        best = jnp.max(functools.reduce(jnp.maximum, parts).reshape(ROWS // 8, 8, width), axis=0)
        top = stat[head, 0:1, lo:hi]
        now = jnp.maximum(top, jnp.max(best, axis=0, keepdims=True))
        es = [jnp.exp(part - now) for part in parts]
        summed = functools.reduce(jnp.add, [jnp.sum(e.reshape(ROWS // 8, 8, width), axis=0) for e in es])
        new = dot_nn(
            jnp.concatenate([kv_buf[i, 2] for i in slots], axis=1),
            jnp.concatenate([e.astype(BF16) for e in es], axis=0),
        )
        keep = jnp.exp(top - now)
        stat[head, 0:1, lo:hi] = now
        stat[head, 1:2, lo:hi] = keep * stat[head, 1:2, lo:hi] + jnp.sum(summed, axis=0, keepdims=True)
        acc[head, :, lo:hi] = keep * acc[head, :, lo:hi] + new

    def early(hop):
        queries, keys = within(hop, ny), within(hop, nz)
        for k in keys:
            when(seen(0, k), lambda k=k: attend(0, queries, [k], False))
        queries, keys = within(hop, nz), within(hop, ny)
        for q in queries:
            when(seen(1, q), lambda q=q: attend(1, [q], keys, False))

    def late_queries(hop):
        keys = within(hop, nz)
        before = [k for k in keys if k <= 0]
        close = [k for k in before if k >= -1]
        if len(close) < len(before) and ring(hop, ny):
            pl.when(z < 2)(lambda: attend(0, ring(hop, ny), close))
            pl.when(z >= 2)(lambda: attend(0, ring(hop, ny), before))
        else:
            attend(0, ring(hop, ny), before)
        rest = [k for k in keys if k > 0]
        if rest and ring(hop, ny):
            pl.when(z + max(rest) >= nz)(lambda: attend(0, ring(hop, ny), rest))
        for q in ring(hop, nz):
            when(seen(1, q), lambda q=q: attend(1, [q], within(hop, ny), False))

    def late_keys(hop):
        for k in ring(hop, nz):
            when(seen(0, k), lambda k=k: attend(0, within(hop - 1, ny), [k], False))
        queries, close = within(hop - 1, nz), within(1, nz)
        if len(close) < len(queries) and ring(hop, ny):
            pl.when(z >= nz - 2)(lambda: attend(1, close, ring(hop, ny)))
            pl.when(z < nz - 2)(lambda: attend(1, queries, ring(hop, ny)))
        else:
            attend(1, queries, ring(hop, ny))

    rings = ((0, y, ny, y_dev), (1, z, nz, z_dev))

    def reach(side, size):
        return (size - 1) // 2 if side == 1 or size == 8 else size // 2

    routes = [
        (head, side, dist) for head, _, size, _ in rings for side in (0, 1) for dist in range(1, reach(side, size) + 1)
    ]
    halves = [(head, side) for head, _, size, _ in rings if size == 8 for side in (0, 1)]

    def send_half(head, side, me, size, dev):
        top, total, num = load_own(head, size // 2, size)
        lanes = slice(side * ROWS, (side + 1) * ROWS)
        at = halves.index((head, side))
        pf_s[at, 0:DV, :] = num[:, lanes].astype(BF16)
        pf_s[at, DV:, :] = pack_stats([top[:, lanes], total[:, lanes]])
        hop = -2 if side == 0 else 2
        remote(pf_s.at[at], pf_r.at[at], pf_send.at[0], pf_recv.at[at], dev((me + size + hop) % size)).start()

    def combine_half(value, head, side, dev, me):
        at = halves.index((head, side))
        remote(pf_r.at[at], pf_r.at[at], pf_send.at[0], pf_recv.at[at], dev(me)).wait_recv()
        lanes = slice(side * ROWS, (side + 1) * ROWS)
        new_top, new_total = unpack_stats(pf_r[at, DV:, :], 2)
        top, total, num = (v[:, lanes] for v in value)
        now = jnp.maximum(top, new_top)
        keep, weight = jnp.exp(top - now), jnp.exp(new_top - now)
        merged = (now, keep * total + weight * new_total, keep * num + weight * pf_r[at, 0:DV, :].astype(F32))
        rest = [v[:, (1 - side) * ROWS:(2 - side) * ROWS] for v in value]
        pairs = zip(merged, rest) if side == 0 else zip(rest, merged)
        return tuple(jnp.concatenate(pair, axis=1) for pair in pairs)

    def load_own(head, off, size):
        lo = arrival(off, size) * 2 * ROWS
        hi = lo + 2 * ROWS
        return stat[head, 0:1, lo:hi], stat[head, 1:2, lo:hi], acc[head, :, lo:hi]

    def combine(one, message):
        top, total, num = one
        t0, l0, t1, l1 = unpack_stats(message[2 * DV:, :])
        new_top = jnp.concatenate([t0, t1], axis=1)
        now = jnp.maximum(top, new_top)
        keep = jnp.exp(top - now)
        weight = jnp.exp(new_top - now)
        new_num = jnp.concatenate([message[0:DV, :].astype(F32), message[DV:2 * DV, :].astype(F32)], axis=1)
        total = keep * total + weight * jnp.concatenate([l0, l1], axis=1)
        return now, total, keep * num + weight * new_num

    def send_partial(head, side, dist, value, me, size, dev):
        way = -1 if side == 0 else 1
        top, total, num = value
        at = routes.index((head, side, dist))
        out = po_s.at[at]
        out[0:DV, :] = num[:, :ROWS].astype(BF16)
        out[DV:2 * DV, :] = num[:, ROWS:].astype(BF16)
        out[2 * DV:, :] = pack_stats([top[:, :ROWS], total[:, :ROWS], top[:, ROWS:], total[:, ROWS:]])
        step = min(dist, 2) if dist < 3 else 1
        remote(
            out, po_r.at[at], po_send.at[0], po_recv.at[at], dev((me + size + way * step) % size)
        ).start()

    def await_partial(head, side, dist, dev, me):
        at = routes.index((head, side, dist))
        remote(po_r.at[at], po_r.at[at], po_send.at[0], po_recv.at[at], dev(me)).wait_recv()
        return po_r.at[at]


    def own_part(head, side, dist, me, size, dev):
        way = -1 if side == 0 else 1
        send_partial(head, side, dist, load_own(head, way * dist, size), me, size, dev)

    def passing(head, side, dist, me, size, dev):
        way = -1 if side == 0 else 1
        value = load_own(head, way * dist, size)
        if size == 8:
            value = combine_half(value, head, side, dev, me)
        for farther in range(dist + 1, reach(side, size) + 1):
            value = combine(value, await_partial(head, side, farther, dev, me))
        send_partial(head, side, dist, value, me, size, dev)

    last_hop = max(ny, nz) // 2
    def keep_arrived(hop):
        for head, size in ((0, ny), (1, nz)):
            for q in ring(hop, size):
                keep_queries(head, q)

    def send_far():
        for head, me, size, dev in rings:
            if size == 8:
                for side in (0, 1):
                    send_half(head, side, me, size, dev)
            elif size // 2 == last_hop:
                own_part(head, 0, reach(0, size), me, size, dev)

    keep_arrived(0)
    first_round = min(1, last_hop - 1)
    if first_round == 0:
        early(0)
    for hop in range(1, last_hop + 1):
        phase("gather_hop" + str(hop))
        pass_on(hop)
        if hop == min(2, last_hop):
            state_send()
        keep_arrived(hop)
        if hop == first_round:
            phase("early")
            early(hop)
        elif hop > first_round:
            phase("late_queries" + str(hop))
            late_queries(hop)
            if hop == last_hop:
                send_far()
            phase("late_keys" + str(hop))
            late_keys(hop)
            if hop == min(3, last_hop):
                state_prefix()
    phase("partials")
    for dist in (3, 1):
        for head, me, size, dev in rings:
            for side in (1, 0):
                unsent = side == 1 or size // 2 < last_hop or size == 8
                if dist == reach(side, size) and unsent or dist == 1 and reach(side, size) > 1:
                    own_part(head, side, dist, me, size, dev)
    state_entry()
    phase("pass_far")
    for side in (1, 0):
        for head, me, size, dev in rings:
            if reach(side, size) > 2:
                passing(head, side, 2, me, size, dev)
            elif reach(side, size) == 2 and size // 2 < last_hop:
                own_part(head, side, 2, me, size, dev)

    def finish(head, value):
        top, total, num = value
        att = num[:, :ROWS] / total[:, :ROWS] - lam_ref[head] * num[:, ROWS:] / total[:, ROWS:]
        att = att * lax.rsqrt(jnp.mean(att * att, axis=0, keepdims=True) + EPS)
        lws_ref[head:head + 1, :] = top[:, :ROWS] + jnp.log(total[:, :ROWS])
        return (att.T * attg_ref[...] * 0.8).astype(BF16)

    phase("rec_result")
    all_of(in_r, ny - 1, in_send.at[0], in_recv.at[0]).wait_recv()
    rec = []
    for h in range(2):
        o = ol_scr[h] + dot_nt(qc_scr[h], in_r[:, h].reshape(DV, DV))
        rec.append(norm_rows(o, recg_ref[...]).astype(BF16))
    rec_rows = jnp.concatenate(rec, axis=1)

    for c in wo_copies:
        c.wait()
    width = wo.shape[2] // PARTS
    for k in range(PARTS):
        half_out[k] = dot_nn(rec_rows, wo[1, :, k * width:(k + 1) * width])

    phase("merge_own")
    values = [load_own(head, 0, size) for head, _, size, _ in rings]
    for dist in (1, 2):
        for head, me, size, dev in rings:
            for side in (1, 0):
                if dist <= reach(side, size):
                    values[head] = combine(values[head], await_partial(head, side, dist, dev, me))
    att = [finish(head, values[head]) for head in (0, 1)]
    att_rows = jnp.concatenate(att, axis=1)

    phase("project_out")
    p_list = []
    for k in range(PARTS):
        cols = slice(k * width, (k + 1) * width)
        part = dot_nn(att_rows, wo[0, :, cols]) + half_out[k]
        pbuf[k] = part.astype(BF16)
        c = remote(pbuf.at[k], prx.at[k], p_send.at[0], p_recv.at[k], {"tp": t_other})
        c.start()
        p_list.append(c)
    for k in range(PARTS):
        p_list[k].wait_recv()
        out_ref[:, k * width:(k + 1) * width] = (pbuf[k].astype(F32) + prx[k].astype(F32)).astype(BF16)

    phase("drain")
    for buf, count, sem in (
        (nrm, 3, a_send.at[0]), (rsend, 3, r_send.at[0]), (rsend2, 3, r_send.at[1]),
        (gy, ny - 1, gy_send.at[0]), (gz, nz - 1, gz_send.at[0]), (st_r, ny - 1, st_send.at[0]),
        (tot_r, nz - 1, tot_send.at[0]), (in_r, ny - 1, in_send.at[0]), (po_s, len(routes), po_send.at[0]),
        (pf_s, len(halves), pf_send.at[0]), (pbuf, PARTS, p_send.at[0]),
    ):
        if count:
            all_of(buf, count, sem, sem).wait_send()
    phase(None)


def on_device(nz, ny, tokens, in_gain, wq, wk, wv, wrq, wrf, wri, lam, lb, scale, attg, recg, wa, wr):
    d = tokens.shape[1]
    out_cols = wa.shape[1]
    any_spec = pl.BlockSpec(memory_space=pl.ANY)
    vmem = pl.BlockSpec(memory_space=pltpu.VMEM)
    smem = pl.BlockSpec(memory_space=pltpu.SMEM)
    slice_rows = DV // ny
    st_rows = 2 * slice_rows + 16
    dma = pltpu.SemaphoreType.DMA
    scratch = [
        pltpu.VMEM((ROWS, d), BF16),
        pltpu.VMEM((COLS, d), BF16),
        pltpu.VMEM((2, wa.shape[0], out_cols), BF16),
        pltpu.VMEM((FS, ROWS, d), BF16),
        pltpu.VMEM((FS, ROWS, FIRST), BF16),
        pltpu.VMEM((FS, ROWS, COLS - FIRST), BF16),
        pltpu.VMEM((3, ROWS, FIRST), BF16),
        pltpu.VMEM((3, ROWS, COLS - FIRST), BF16),
        pltpu.VMEM((ny, 3, ROWS, DV), BF16),
        pltpu.VMEM((nz, 3, ROWS, DV), BF16),
        pltpu.VMEM((2, DV, max(ny, nz) * 2 * ROWS), F32),
        pltpu.VMEM((2, 8, max(ny, nz) * 2 * ROWS), F32),
        pltpu.VMEM((2, DV, max(ny, nz) * 2 * ROWS), BF16),
        pltpu.VMEM((12, 2 * DV + 16, ROWS), BF16),
        pltpu.VMEM((12, 2 * DV + 16, ROWS), BF16),
        pltpu.VMEM((4, DV + 16, ROWS), BF16),
        pltpu.VMEM((4, DV + 16, ROWS), BF16),
        pltpu.VMEM((ny, st_rows, DV), BF16),
        pltpu.VMEM((ny, st_rows, DV), BF16),
        pltpu.VMEM((st_rows, DV), BF16),
        pltpu.VMEM((nz, st_rows, DV), BF16),
        pltpu.VMEM((ny, 2, slice_rows, DV), BF16),
        pltpu.VMEM((ny, 2, slice_rows, DV), BF16),
        pltpu.VMEM((ny, st_rows, DV), F32),
        pltpu.VMEM((2, ROWS, DV), BF16),
        pltpu.VMEM((2, ROWS, DV), F32),
        pltpu.VMEM((PARTS, ROWS, out_cols // PARTS), BF16),
        pltpu.VMEM((PARTS, ROWS, out_cols // PARTS), BF16),
        pltpu.VMEM((PARTS, ROWS, out_cols // PARTS), F32),
        dma((9,)), dma((1,)), dma((FS, 4)), dma((2,)), dma((2,)),
        dma((1,)), dma((ny, 3)), dma((1,)), dma((nz, 3)),
        dma((1,)), dma((12,)), dma((1,)), dma((4,)),
        dma((1,)), dma((1,)), dma((1,)), dma((1,)), dma((1,)), dma((1,)),
        dma((1,)), dma((PARTS,)),
    ]
    mixed, log_sum = pl.pallas_call(
        functools.partial(kernel_body, nz, ny),
        out_shape=(pltpu.VMEM((ROWS, out_cols), BF16), pltpu.VMEM((2, ROWS), F32)),
        in_specs=[any_spec, vmem] + [any_spec] * 6 + [smem, vmem, vmem, vmem, vmem, any_spec, any_spec],
        out_specs=(vmem, vmem),
        scratch_shapes=scratch,
        compiler_params=pltpu.CompilerParams(
            collective_id=0, has_side_effects=True, vmem_limit_bytes=56 * 1024 * 1024
        ),
    )(
        tokens, in_gain.reshape(1, d), wq.T, wk.T, wv.T, wrq.T, wrf.T, wri.T, lam, lb,
        scale.reshape(1, ROWS), attg.reshape(1, DV), recg.reshape(1, DV), wa, wr,
    )
    return mixed, log_sum


def plane_of(size):
    nz = 1
    while nz * nz < size:
        nz *= 2
    return nz, size // nz


def solution(mesh):
    nz, ny = plane_of(mesh.shape["sp"])
    col_split = P(None, ("tp", "fs"))
    placed = (
        P(("fs", "sp"), None), P(),
        col_split, col_split, col_split, col_split, col_split, col_split,
        P("tp"), P("tp", None), P(("fs", "sp")), P(), P(),
        P("tp", None), P("tp", None),
    )
    return jax.shard_map(
        functools.partial(on_device, nz, ny),
        mesh=mesh,
        in_specs=placed,
        out_specs=(P(("fs", "sp"), None), P("tp", ("fs", "sp"))),
        check_vma=False,
    )
```

```python
import functools

import jax
import jax.numpy as jnp
from jax import lax
from jax.experimental import pallas as pl
from jax.experimental.pallas import tpu as pltpu
from jax.sharding import PartitionSpec as P

DK = 64
DV = 128
ROWS = 128
COLS = 384
FIRST = 256
EPS = 1e-06
NEG = -1e30
FS = 4
PARTS = 4
MESH = pl.DeviceIdType.MESH
F32 = jnp.float32
BF16 = jnp.bfloat16


def dot_nn(a, b):
    return lax.dot_general(a, b, (((1,), (0,)), ((), ())), preferred_element_type=F32)


def dot_nt(a, b):
    return lax.dot_general(a, b, (((1,), (1,)), ((), ())), preferred_element_type=F32)


def pack_rates(first, second):
    parts = []
    for rate in (first, second):
        high = rate.astype(BF16).astype(F32)
        parts += [jnp.broadcast_to(v, (4, DV)) for v in (high, rate - high)]
    return jnp.concatenate(parts, axis=0).astype(BF16)


def unpack_rates(packed):
    wide = packed.astype(F32)
    return wide[0:1] + wide[4:5], wide[8:9] + wide[12:13]


def pack_stats(rows):
    tile = jnp.zeros((16, DV), F32)
    where = lax.broadcasted_iota(jnp.int32, (16, DV), 0)
    for i, value in enumerate(rows):
        high = value.astype(BF16).astype(F32)
        middle = (value - high).astype(BF16).astype(F32)
        for j, part in enumerate((high, middle, value - high - middle)):
            tile = jnp.where(where == 3 * i + j, part, tile)
    return tile.astype(BF16)


def unpack_stats(packed, count=4):
    wide = packed.astype(F32)
    return [wide[3 * i:3 * i + 1] + wide[3 * i + 1:3 * i + 2] + wide[3 * i + 2:3 * i + 3] for i in range(count)]


def norm_rows(values, gain):
    mean = jnp.mean(values * values, axis=-1, keepdims=True)
    return values * lax.rsqrt(mean + EPS) * gain


def kernel_body(
    nz, ny,
    tok_hbm, gain_ref, wq, wk, wv, wrq, wrf, wri, lam_ref, lb_ref, scale_ref, attg_ref, recg_ref,
    wa_hbm, wr_hbm,
    out_ref, lws_ref,
    tok, wcat, wo, nrm, res, res2, rsend, rsend2,
    gy, gz, acc, stat, qb, po_s, po_r, pf_s, pf_r,
    st_s, st_r, tot_s, tot_r, in_s, in_r, pref, qc_scr, ol_scr,
    pbuf, prx, half_out,
    lsem, a_send, a_recv, r_send, r_recv,
    gy_send, gy_recv, gz_send, gz_recv,
    po_send, po_recv, pf_send, pf_recv,
    st_send, st_recv, tot_send, tot_recv, in_send, in_recv,
    p_send, p_recv,
):
    p = lax.axis_index("sp")
    x = lax.axis_index("fs")
    t = lax.axis_index("tp")
    z = p // ny
    y = p % ny
    t_other = 1 - t
    xl = (x + 3) % 4
    xr = (x + 1) % 4
    xo = (x + 2) % 4
    slice_rows = DV // ny

    open_scope = []

    def phase(name):
        if open_scope:
            open_scope.pop().__exit__(None, None, None)
        if name:
            scope = jax.named_scope(name)
            scope.__enter__()
            open_scope.append(scope)

    phase("start")
    weights = (wq, wk, wv, wrq, wrf, wri)
    tok_copy = pltpu.make_async_copy(tok_hbm, tok, lsem.at[0])
    tok_copy.start()
    w_copies = [
        pltpu.make_async_copy(w, wcat.at[pl.ds(i * DK, DK)], lsem.at[1 + i]) for i, w in enumerate(weights)
    ]
    for c in w_copies:
        c.start()
    wo_copies = [
        pltpu.make_async_copy(wa_hbm, wo.at[0], lsem.at[7]),
        pltpu.make_async_copy(wr_hbm, wo.at[1], lsem.at[8]),
    ]
    for c in wo_copies:
        c.start()

    barrier = pltpu.get_barrier_semaphore()

    def greet(dev):
        pl.semaphore_signal(barrier, inc=1, device_id=dev, device_id_type=MESH)

    greet({"tp": t_other})
    for d in range(1, 4):
        greet({"fs": (x + d) % 4})
    for d in range(1, ny):
        greet({"sp": z * ny + (y + d) % ny})
    for d in range(1, nz):
        greet({"sp": ((z + d) % nz) * ny + y})

    def remote(src, dst, ssem, rsem, dev):
        return pltpu.make_async_remote_copy(
            src_ref=src, dst_ref=dst, send_sem=ssem, recv_sem=rsem, device_id=dev, device_id_type=MESH
        )

    def piece(f, tt, pc):
        return nrm.at[f, pl.ds(pl.multiple_of(tt * 64 + pc * 32, 32), 32)]

    def a_sem(f, tt, pc):
        return a_recv.at[f, tt * 2 + pc]

    def normalise(tt, pc):
        rows = pl.ds(pl.multiple_of(tt * 64 + pc * 32, 32), 32)
        nrm[x, rows, :] = norm_rows(tok[rows, :].astype(F32), gain_ref[...]).astype(BF16)

    tok_copy.wait()
    normalise(t, 0)
    normalise(t, 1)
    phase("entry_barrier")
    pl.semaphore_wait(barrier, 1 + 3 + (ny - 1) + (nz - 1))

    def a_start(k, f, pc, dev):
        c = remote(piece(f, t, pc), piece(f, t, pc), a_send.at[0], a_sem(f, t, pc), dev)
        c.start()

    def a_wait(f, tt, pc):
        remote(piece(f, tt, pc), piece(f, tt, pc), a_send.at[0], a_sem(f, tt, pc), {"fs": xr}).wait_recv()

    phase("x_own")
    a_start(0, x, 0, {"fs": xr})
    a_start(1, x, 1, {"fs": xl})
    a_start(2, x, 1, {"fs": xr})
    a_start(3, x, 0, {"fs": xl})
    normalise(t_other, 0)
    normalise(t_other, 1)
    for i in range(6):
        w_copies[i].wait()

    def project(rows):
        return dot_nt(rows, wcat[...]).astype(BF16)

    acc[...] = jnp.zeros_like(acc)
    stat[...] = jnp.full(stat.shape, NEG, F32)
    own = project(nrm[x])
    res[x] = own[:, :FIRST]
    res2[x] = own[:, FIRST:]
    phase("x_forward")
    a_wait(xl, t, 0)
    a_start(4, xl, 0, {"fs": xr})
    a_start(5, xl, 0, {"tp": t_other})
    a_wait(xr, t, 1)
    a_start(6, xr, 1, {"fs": xl})
    a_start(7, xr, 1, {"tp": t_other})
    a_wait(xl, t, 1)
    a_start(8, xl, 1, {"tp": t_other})
    a_wait(xr, t, 0)
    a_start(9, xr, 0, {"tp": t_other})

    def answer(k, f):
        for j, (out, into) in enumerate(((rsend, res), (rsend2, res2))):
            remote(out.at[k], into.at[x], r_send.at[j], r_recv.at[j], {"fs": f}).start()

    phase("x_near")
    for f in (xl, xr):
        a_wait(f, t_other, 0)
        a_wait(f, t_other, 1)
    near = project(jnp.concatenate([nrm[xl], nrm[xr]], axis=0))
    for k in (0, 1):
        rsend[k] = near[k * ROWS:(k + 1) * ROWS, :FIRST]
        rsend2[k] = near[k * ROWS:(k + 1) * ROWS, FIRST:]
    answer(0, xl)
    answer(1, xr)
    phase("x_far")
    a_wait(xo, t, 0)
    a_start(10, xo, 0, {"tp": t_other})
    a_wait(xo, t, 1)
    a_start(11, xo, 1, {"tp": t_other})
    a_wait(xo, t_other, 0)
    a_wait(xo, t_other, 1)
    far = project(nrm[xo])
    rsend[2] = far[:, :FIRST]
    rsend2[2] = far[:, FIRST:]
    answer(2, xo)
    phase("x_answers")
    def all_of(buf, count, send, recv):
        part = buf.at[pl.ds(0, count)]
        return remote(part, part, send, recv, {"tp": t_other})

    all_of(res, 3, r_send.at[0], r_recv.at[0]).wait_recv()

    phase("tiles")
    def tile(kind, h):
        lo, ref = (kind * DK, res) if kind * DK < FIRST else (kind * DK - FIRST, res2)
        return jnp.concatenate([ref[2 * h, :, lo:lo + DK], ref[2 * h + 1, :, lo:lo + DK]], axis=1)

    def value_t(h):
        return tile(2, h).astype(F32).T.astype(BF16)

    scale_q = jnp.asarray(DK ** (-0.5), BF16)
    gy[0, 0] = (tile(0, 0) * scale_q).astype(F32).T.astype(BF16)
    gy[0, 1] = tile(1, 1)
    gy[0, 2] = value_t(1)
    gz[0, 0] = (tile(0, 1) * scale_q).astype(F32).T.astype(BF16)
    gz[0, 1] = tile(1, 0)
    gz[0, 2] = value_t(0)

    def y_dev(yy):
        return {"sp": z * ny + yy}

    def z_dev(zz):
        return {"sp": zz * ny + y}

    def pass_on(hop):
        for k in range(3):
            for buf, sent, got, me, size, dev in (
                (gy, gy_send, gy_recv, y, ny, y_dev), (gz, gz_send, gz_recv, z, nz, z_dev)
            ):
                for way in (1, -1):
                    def carried(h):
                        return 2 * h < size or (2 * h == size and (k % 2 == 0) == (way == 1))

                    here = (-way * hop) % size
                    there = (-way * (hop + 1)) % size
                    dev_next = dev((me + size + way) % size)
                    if hop > 0 and carried(hop):
                        remote(buf.at[here, k], buf.at[here, k], sent.at[0], got.at[here, k], dev_next).wait_recv()
                    if carried(hop + 1):
                        remote(buf.at[here, k], buf.at[there, k], sent.at[0], got.at[there, k], dev_next).start()

    pass_on(0)

    phase("rec_local")
    all_of(res2, 3, r_send.at[1], r_recv.at[1]).wait_recv()
    row = lax.broadcasted_iota(jnp.int32, (ROWS, ROWS), 0)
    col = lax.broadcasted_iota(jnp.int32, (ROWS, ROWS), 1)
    tril = jnp.where(row >= col, 1.0, 0.0).astype(F32)
    rates = []
    scale_col = jnp.broadcast_to(scale_ref[...], (ROWS, ROWS)).T
    for h in range(2):
        rq = tile(3, h).astype(F32)
        rf = tile(4, h).astype(F32)
        ri = tile(5, h)
        edge = lb_ref[h:h + 1, :]
        forget = edge + (1.0 - edge) * jax.nn.sigmoid(rf)
        g = scale_col * jnp.log(forget)
        kk = 1.0 - jnp.exp(g)
        cum = lax.dot_general(
            tril, g, (((1,), (0,)), ((), ())), precision=lax.Precision.HIGHEST, preferred_element_type=F32
        )
        scores = jnp.where(row == col, jnp.sum(rq * kk, axis=-1, keepdims=True), 0.0)
        c8 = cum.reshape(ROWS // 8, 8, DV)
        r8 = lax.broadcasted_iota(jnp.int32, (ROWS // 8, 8, DV), 1)
        for b in (64, 32, 16, 8, 4, 2, 1):
            if b >= 8:
                c3 = cum.reshape(ROWS // (2 * b), 2 * b, DV)
                diff = (c3 - c3[:, b - 1:b, :]).reshape(ROWS, DV)
            else:
                mid = c8[:, b - 1:b, :]
                for first in range(2 * b, 8, 2 * b):
                    mid = jnp.where(r8 >= first, c8[:, first + b - 1:first + b, :], mid)
                diff = (c8 - mid).reshape(ROWS, DV)
            upper = (row & (2 * b - 1)) >= b
            decay = jnp.exp(jnp.where(upper, diff, -diff))
            late = jnp.where(upper, rq * decay, 0.0).astype(BF16)
            early = jnp.where(upper, 0.0, kk * decay).astype(BF16)
            level = dot_nt(late, early)
            scores = scores + jnp.where((row ^ col) < 2 * b, level, 0.0)
        ol_scr[h] = dot_nn(scores.astype(BF16), ri)
        last = cum[ROWS - 1:ROWS, :]
        key_end = (kk * jnp.exp(last - cum)).astype(BF16)
        state_t = dot_nn(ri.astype(F32).T.astype(BF16), key_end)
        qc_scr[h] = (rq * jnp.exp(cum)).astype(BF16)
        st_s[:, h * slice_rows:(h + 1) * slice_rows, :] = state_t.reshape(ny, slice_rows, DV).astype(BF16)
        rates.append(jnp.exp(last))
    packed = pack_rates(*rates)
    for k in range(ny):
        st_s[k, 2 * slice_rows:, :] = packed
    def state_send():
        st_r[y] = st_s[y]
        for d in range(1, ny):
            yy = (y + d) % ny
            remote(st_s.at[yy], st_r.at[y], st_send.at[0], st_recv.at[0], y_dev(yy)).start()

    half = slice_rows

    def step_of(ref):
        d0, d1 = unpack_rates(ref[2 * half:, :])
        return d0, ref[0:half, :].astype(F32), d1, ref[half:2 * half, :].astype(F32)

    def state_prefix():
        phase("rec_prefix")
        all_of(st_r, ny - 1, st_send.at[0], st_recv.at[0]).wait_recv()

        s0 = s1 = jnp.zeros((half, DV), F32)
        c0 = c1 = jnp.ones((1, DV), F32)
        for k in range(ny):
            pref[k, 0:half, :] = s0
            pref[k, half:2 * half, :] = s1
            pref[k, 2 * half:2 * half + 8, :] = jnp.broadcast_to(c0, (8, DV))
            pref[k, 2 * half + 8:2 * half + 16, :] = jnp.broadcast_to(c1, (8, DV))
            d0, a0, d1, a1 = step_of(st_r.at[k])
            s0, s1, c0, c1 = d0 * s0 + a0, d1 * s1 + a1, c0 * d0, c1 * d1
        tot_s[0:half, :] = s0.astype(BF16)
        tot_s[half:2 * half, :] = s1.astype(BF16)
        tot_s[2 * half:, :] = pack_rates(c0, c1)
        for d in range(1, nz):
            zz = (z + d) % nz
            remote(tot_s, tot_r.at[z], tot_send.at[0], tot_recv.at[0], z_dev(zz)).start()

    def state_entry():
        phase("rec_totals")
        all_of(tot_r, nz - 1, tot_send.at[0], tot_recv.at[0]).wait_recv()

        def fold(k, carry):
            d0, a0, d1, a1 = step_of(tot_r.at[k])
            return (d0 * carry[0] + a0, d1 * carry[1] + a1)

        entry = lax.fori_loop(0, z, fold, (jnp.zeros((half, DV), F32), jnp.zeros((half, DV), F32)))
        for k in range(ny):
            for h in range(2):
                d = pref[k, 2 * half + 8 * h:2 * half + 8 * h + 1, :]
                in_s[k, h] = (d * entry[h] + pref[k, h * half:(h + 1) * half, :]).astype(BF16)
        in_r[y] = in_s[y]
        for d in range(1, ny):
            yy = (y + d) % ny
            remote(in_s.at[yy], in_r.at[y], in_send.at[0], in_recv.at[0], y_dev(yy)).start()

    channel = lax.broadcasted_iota(jnp.int32, (ROWS, DV), 0)
    below = (
        lax.broadcasted_iota(jnp.int32, (ROWS, 2 * ROWS), 0)
        <= (lax.broadcasted_iota(jnp.int32, (ROWS, 2 * ROWS), 1) & (ROWS - 1))
    )

    def seen(head, off):
        if off % nz == 0:
            return None
        other = (z + off % nz) % nz
        return other < z if head == 0 else other > z

    def when(condition, body):
        if condition is None:
            body()
        else:
            pl.when(condition)(body)

    def ring(hop, size):
        if hop == 0:
            return [0]
        if 2 * hop < size:
            return [hop, -hop]
        return [hop] if 2 * hop == size else []

    def within(hop, size):
        return [o for h in range(hop + 1) for o in ring(h, size)]

    def arrival(off, size):
        return [o % size for o in within(size, size)].index(off % size)

    def sides(head):
        return (gy, gz, ny, nz) if head == 0 else (gz, gy, nz, ny)

    def keep_queries(head, off):
        q_buf, _, q_size, _ = sides(head)
        queries = q_buf[off % q_size, 0]
        zero = jnp.zeros_like(queries)
        at = arrival(off, q_size) * 2 * ROWS
        qb[head, :, at:at + ROWS] = jnp.where(channel < DK, queries, zero)
        qb[head, :, at + ROWS:at + 2 * ROWS] = jnp.where(channel < DK, zero, queries)

    def hidden(head, q_off, k_off):
        _, _, q_size, k_size = sides(head)
        if head == 0:
            if k_off % nz == 0:
                return y > (y + q_off % ny) % ny
            return (z + k_off % nz) % nz > z
        if q_off % nz == 0:
            return (y + k_off % ny) % ny > y
        return (z + q_off % nz) % nz < z

    def attend(head, q_offs, k_offs, checked=True):
        _, kv_buf, q_size, k_size = sides(head)
        if not q_offs or not k_offs:
            return
        lo = arrival(q_offs[0], q_size) * 2 * ROWS
        hi = lo + len(q_offs) * 2 * ROWS
        slots = [o % k_size for o in k_offs]
        s = dot_nn(jnp.concatenate([kv_buf[i, 1] for i in slots], axis=0), qb[head, :, lo:hi])
        parts = []
        for i, k_off in enumerate(k_offs):
            part = s[i * ROWS:(i + 1) * ROWS]
            blocks = []
            for j, q_off in enumerate(q_offs):
                block = part[:, j * 2 * ROWS:(j + 1) * 2 * ROWS]
                if q_off % q_size == 0 and k_off % k_size == 0:
                    block = jnp.where(below, block, NEG)
                elif checked or (k_off if head == 0 else q_off) % nz == 0:
                    block = block + jnp.where(hidden(head, q_off, k_off), NEG, 0.0).astype(F32)
                blocks.append(block)
            parts.append(jnp.concatenate(blocks, axis=1))
        width = hi - lo
        best = jnp.max(functools.reduce(jnp.maximum, parts).reshape(ROWS // 8, 8, width), axis=0)
        top = stat[head, 0:1, lo:hi]
        now = jnp.maximum(top, jnp.max(best, axis=0, keepdims=True))
        es = [jnp.exp(part - now) for part in parts]
        summed = functools.reduce(jnp.add, [jnp.sum(e.reshape(ROWS // 8, 8, width), axis=0) for e in es])
        new = dot_nn(
            jnp.concatenate([kv_buf[i, 2] for i in slots], axis=1),
            jnp.concatenate([e.astype(BF16) for e in es], axis=0),
        )
        keep = jnp.exp(top - now)
        stat[head, 0:1, lo:hi] = now
        stat[head, 1:2, lo:hi] = keep * stat[head, 1:2, lo:hi] + jnp.sum(summed, axis=0, keepdims=True)
        acc[head, :, lo:hi] = keep * acc[head, :, lo:hi] + new

    def early(hop):
        queries, keys = within(hop, ny), within(hop, nz)
        for k in keys:
            when(seen(0, k), lambda k=k: attend(0, queries, [k], False))
        queries, keys = within(hop, nz), within(hop, ny)
        for q in queries:
            when(seen(1, q), lambda q=q: attend(1, [q], keys, False))

    def late_queries(hop):
        keys = within(hop, nz)
        before = [k for k in keys if k <= 0]
        close = [k for k in before if k >= -1]
        if len(close) < len(before) and ring(hop, ny):
            pl.when(z < 2)(lambda: attend(0, ring(hop, ny), close))
            pl.when(z >= 2)(lambda: attend(0, ring(hop, ny), before))
        else:
            attend(0, ring(hop, ny), before)
        rest = [k for k in keys if k > 0]
        if rest and ring(hop, ny):
            pl.when(z + max(rest) >= nz)(lambda: attend(0, ring(hop, ny), rest))
        for q in ring(hop, nz):
            when(seen(1, q), lambda q=q: attend(1, [q], within(hop, ny), False))

    def late_keys(hop):
        for k in ring(hop, nz):
            when(seen(0, k), lambda k=k: attend(0, within(hop - 1, ny), [k], False))
        queries, close = within(hop - 1, nz), within(1, nz)
        if len(close) < len(queries) and ring(hop, ny):
            pl.when(z >= nz - 2)(lambda: attend(1, close, ring(hop, ny)))
            pl.when(z < nz - 2)(lambda: attend(1, queries, ring(hop, ny)))
        else:
            attend(1, queries, ring(hop, ny))

    rings = ((0, y, ny, y_dev), (1, z, nz, z_dev))

    def reach(side, size):
        return (size - 1) // 2 if side == 1 or size == 8 else size // 2

    routes = [
        (head, side, dist) for head, _, size, _ in rings for side in (0, 1) for dist in range(1, reach(side, size) + 1)
    ]
    halves = [(head, side) for head, _, size, _ in rings if size == 8 for side in (0, 1)]

    def send_half(head, side, me, size, dev):
        top, total, num = load_own(head, size // 2, size)
        lanes = slice(side * ROWS, (side + 1) * ROWS)
        at = halves.index((head, side))
        pf_s[at, 0:DV, :] = num[:, lanes].astype(BF16)
        pf_s[at, DV:, :] = pack_stats([top[:, lanes], total[:, lanes]])
        hop = -2 if side == 0 else 2
        remote(pf_s.at[at], pf_r.at[at], pf_send.at[0], pf_recv.at[at], dev((me + size + hop) % size)).start()

    def combine_half(value, head, side, dev, me):
        at = halves.index((head, side))
        remote(pf_r.at[at], pf_r.at[at], pf_send.at[0], pf_recv.at[at], dev(me)).wait_recv()
        lanes = slice(side * ROWS, (side + 1) * ROWS)
        new_top, new_total = unpack_stats(pf_r[at, DV:, :], 2)
        top, total, num = (v[:, lanes] for v in value)
        now = jnp.maximum(top, new_top)
        keep, weight = jnp.exp(top - now), jnp.exp(new_top - now)
        merged = (now, keep * total + weight * new_total, keep * num + weight * pf_r[at, 0:DV, :].astype(F32))
        rest = [v[:, (1 - side) * ROWS:(2 - side) * ROWS] for v in value]
        pairs = zip(merged, rest) if side == 0 else zip(rest, merged)
        return tuple(jnp.concatenate(pair, axis=1) for pair in pairs)

    def load_own(head, off, size):
        lo = arrival(off, size) * 2 * ROWS
        hi = lo + 2 * ROWS
        return stat[head, 0:1, lo:hi], stat[head, 1:2, lo:hi], acc[head, :, lo:hi]

    def combine(one, message):
        top, total, num = one
        t0, l0, t1, l1 = unpack_stats(message[2 * DV:, :])
        new_top = jnp.concatenate([t0, t1], axis=1)
        now = jnp.maximum(top, new_top)
        keep = jnp.exp(top - now)
        weight = jnp.exp(new_top - now)
        new_num = jnp.concatenate([message[0:DV, :].astype(F32), message[DV:2 * DV, :].astype(F32)], axis=1)
        total = keep * total + weight * jnp.concatenate([l0, l1], axis=1)
        return now, total, keep * num + weight * new_num

    def send_partial(head, side, dist, value, me, size, dev):
        way = -1 if side == 0 else 1
        top, total, num = value
        at = routes.index((head, side, dist))
        out = po_s.at[at]
        out[0:DV, :] = num[:, :ROWS].astype(BF16)
        out[DV:2 * DV, :] = num[:, ROWS:].astype(BF16)
        out[2 * DV:, :] = pack_stats([top[:, :ROWS], total[:, :ROWS], top[:, ROWS:], total[:, ROWS:]])
        step = min(dist, 2) if dist < 3 else 1
        remote(
            out, po_r.at[at], po_send.at[0], po_recv.at[at], dev((me + size + way * step) % size)
        ).start()

    def await_partial(head, side, dist, dev, me):
        at = routes.index((head, side, dist))
        remote(po_r.at[at], po_r.at[at], po_send.at[0], po_recv.at[at], dev(me)).wait_recv()
        return po_r.at[at]


    def own_part(head, side, dist, me, size, dev):
        way = -1 if side == 0 else 1
        send_partial(head, side, dist, load_own(head, way * dist, size), me, size, dev)

    def passing(head, side, dist, me, size, dev):
        way = -1 if side == 0 else 1
        value = load_own(head, way * dist, size)
        if size == 8:
            value = combine_half(value, head, side, dev, me)
        for farther in range(dist + 1, reach(side, size) + 1):
            value = combine(value, await_partial(head, side, farther, dev, me))
        send_partial(head, side, dist, value, me, size, dev)

    last_hop = max(ny, nz) // 2
    def keep_arrived(hop):
        for head, size in ((0, ny), (1, nz)):
            for q in ring(hop, size):
                keep_queries(head, q)

    def send_far():
        for head, me, size, dev in rings:
            if size == 8:
                for side in (0, 1):
                    send_half(head, side, me, size, dev)
            elif size // 2 == last_hop:
                own_part(head, 0, reach(0, size), me, size, dev)

    keep_arrived(0)
    first_round = min(1, last_hop - 1)
    if first_round == 0:
        early(0)
    for hop in range(1, last_hop + 1):
        phase("gather_hop" + str(hop))
        pass_on(hop)
        if hop == min(2, last_hop):
            state_send()
        keep_arrived(hop)
        if hop == first_round:
            phase("early")
            early(hop)
        elif hop > first_round:
            phase("late_queries" + str(hop))
            late_queries(hop)
            if hop == last_hop:
                send_far()
            phase("late_keys" + str(hop))
            late_keys(hop)
            if hop == min(3, last_hop):
                state_prefix()
    phase("partials")
    for dist in (3, 1):
        for head, me, size, dev in rings:
            for side in (1, 0):
                unsent = side == 1 or size // 2 < last_hop or size == 8
                if dist == reach(side, size) and unsent or dist == 1 and reach(side, size) > 1:
                    own_part(head, side, dist, me, size, dev)
    state_entry()
    phase("pass_far")
    for side in (1, 0):
        for head, me, size, dev in rings:
            if reach(side, size) > 2:
                passing(head, side, 2, me, size, dev)
            elif reach(side, size) == 2 and size // 2 < last_hop:
                own_part(head, side, 2, me, size, dev)

    def finish(head, value):
        top, total, num = value
        att = num[:, :ROWS] / total[:, :ROWS] - lam_ref[head] * num[:, ROWS:] / total[:, ROWS:]
        att = att * lax.rsqrt(jnp.mean(att * att, axis=0, keepdims=True) + EPS)
        lws_ref[head:head + 1, :] = top[:, :ROWS] + jnp.log(total[:, :ROWS])
        return (att.T * attg_ref[...] * 0.8).astype(BF16)

    def own_merged(head, dist, value):
        _, me, size, dev = rings[head]
        for side in (1, 0):
            if dist <= reach(side, size):
                value = combine(value, await_partial(head, side, dist, dev, me))
        return value

    phase("merge_near")
    for head, _, size, _ in rings:
        top, total, num = own_merged(head, 1, load_own(head, 0, size))
        stat[head, 2:3, :2 * ROWS] = top
        stat[head, 3:4, :2 * ROWS] = total
        acc[head, :, :2 * ROWS] = num
    phase("rec_result")
    all_of(in_r, ny - 1, in_send.at[0], in_recv.at[0]).wait_recv()
    rec = []
    for h in range(2):
        o = ol_scr[h] + dot_nt(qc_scr[h], in_r[:, h].reshape(DV, DV))
        rec.append(norm_rows(o, recg_ref[...]).astype(BF16))
    rec_rows = jnp.concatenate(rec, axis=1)

    for c in wo_copies:
        c.wait()
    width = wo.shape[2] // PARTS
    for k in range(PARTS):
        half_out[k] = dot_nn(rec_rows, wo[1, :, k * width:(k + 1) * width])

    phase("merge_own")
    values = [own_merged(head, 2, (stat[head, 2:3, :2 * ROWS], stat[head, 3:4, :2 * ROWS], acc[head, :, :2 * ROWS]))
              for head in (0, 1)]
    att = [finish(head, values[head]) for head in (0, 1)]
    att_rows = jnp.concatenate(att, axis=1)

    phase("project_out")
    p_list = []
    for k in range(PARTS):
        cols = slice(k * width, (k + 1) * width)
        part = dot_nn(att_rows, wo[0, :, cols]) + half_out[k]
        pbuf[k] = part.astype(BF16)
        c = remote(pbuf.at[k], prx.at[k], p_send.at[0], p_recv.at[k], {"tp": t_other})
        c.start()
        p_list.append(c)
    for k in range(PARTS):
        p_list[k].wait_recv()
        out_ref[:, k * width:(k + 1) * width] = (pbuf[k].astype(F32) + prx[k].astype(F32)).astype(BF16)

    phase("drain")
    for buf, count, sem in (
        (nrm, 3, a_send.at[0]), (rsend, 3, r_send.at[0]), (rsend2, 3, r_send.at[1]),
        (gy, ny - 1, gy_send.at[0]), (gz, nz - 1, gz_send.at[0]), (st_r, ny - 1, st_send.at[0]),
        (tot_r, nz - 1, tot_send.at[0]), (in_r, ny - 1, in_send.at[0]), (po_s, len(routes), po_send.at[0]),
        (pf_s, len(halves), pf_send.at[0]), (pbuf, PARTS, p_send.at[0]),
    ):
        if count:
            all_of(buf, count, sem, sem).wait_send()
    phase(None)


def on_device(nz, ny, tokens, in_gain, wq, wk, wv, wrq, wrf, wri, lam, lb, scale, attg, recg, wa, wr):
    d = tokens.shape[1]
    out_cols = wa.shape[1]
    any_spec = pl.BlockSpec(memory_space=pl.ANY)
    vmem = pl.BlockSpec(memory_space=pltpu.VMEM)
    smem = pl.BlockSpec(memory_space=pltpu.SMEM)
    slice_rows = DV // ny
    st_rows = 2 * slice_rows + 16
    dma = pltpu.SemaphoreType.DMA
    scratch = [
        pltpu.VMEM((ROWS, d), BF16),
        pltpu.VMEM((COLS, d), BF16),
        pltpu.VMEM((2, wa.shape[0], out_cols), BF16),
        pltpu.VMEM((FS, ROWS, d), BF16),
        pltpu.VMEM((FS, ROWS, FIRST), BF16),
        pltpu.VMEM((FS, ROWS, COLS - FIRST), BF16),
        pltpu.VMEM((3, ROWS, FIRST), BF16),
        pltpu.VMEM((3, ROWS, COLS - FIRST), BF16),
        pltpu.VMEM((ny, 3, ROWS, DV), BF16),
        pltpu.VMEM((nz, 3, ROWS, DV), BF16),
        pltpu.VMEM((2, DV, max(ny, nz) * 2 * ROWS), F32),
        pltpu.VMEM((2, 8, max(ny, nz) * 2 * ROWS), F32),
        pltpu.VMEM((2, DV, max(ny, nz) * 2 * ROWS), BF16),
        pltpu.VMEM((12, 2 * DV + 16, ROWS), BF16),
        pltpu.VMEM((12, 2 * DV + 16, ROWS), BF16),
        pltpu.VMEM((4, DV + 16, ROWS), BF16),
        pltpu.VMEM((4, DV + 16, ROWS), BF16),
        pltpu.VMEM((ny, st_rows, DV), BF16),
        pltpu.VMEM((ny, st_rows, DV), BF16),
        pltpu.VMEM((st_rows, DV), BF16),
        pltpu.VMEM((nz, st_rows, DV), BF16),
        pltpu.VMEM((ny, 2, slice_rows, DV), BF16),
        pltpu.VMEM((ny, 2, slice_rows, DV), BF16),
        pltpu.VMEM((ny, st_rows, DV), F32),
        pltpu.VMEM((2, ROWS, DV), BF16),
        pltpu.VMEM((2, ROWS, DV), F32),
        pltpu.VMEM((PARTS, ROWS, out_cols // PARTS), BF16),
        pltpu.VMEM((PARTS, ROWS, out_cols // PARTS), BF16),
        pltpu.VMEM((PARTS, ROWS, out_cols // PARTS), F32),
        dma((9,)), dma((1,)), dma((FS, 4)), dma((2,)), dma((2,)),
        dma((1,)), dma((ny, 3)), dma((1,)), dma((nz, 3)),
        dma((1,)), dma((12,)), dma((1,)), dma((4,)),
        dma((1,)), dma((1,)), dma((1,)), dma((1,)), dma((1,)), dma((1,)),
        dma((1,)), dma((PARTS,)),
    ]
    mixed, log_sum = pl.pallas_call(
        functools.partial(kernel_body, nz, ny),
        out_shape=(pltpu.VMEM((ROWS, out_cols), BF16), pltpu.VMEM((2, ROWS), F32)),
        in_specs=[any_spec, vmem] + [any_spec] * 6 + [smem, vmem, vmem, vmem, vmem, any_spec, any_spec],
        out_specs=(vmem, vmem),
        scratch_shapes=scratch,
        compiler_params=pltpu.CompilerParams(
            collective_id=0, has_side_effects=True, vmem_limit_bytes=56 * 1024 * 1024
        ),
    )(
        tokens, in_gain.reshape(1, d), wq.T, wk.T, wv.T, wrq.T, wrf.T, wri.T, lam, lb,
        scale.reshape(1, ROWS), attg.reshape(1, DV), recg.reshape(1, DV), wa, wr,
    )
    return mixed, log_sum


def plane_of(size):
    nz = 1
    while nz * nz < size:
        nz *= 2
    return nz, size // nz


def solution(mesh):
    nz, ny = plane_of(mesh.shape["sp"])
    col_split = P(None, ("tp", "fs"))
    placed = (
        P(("fs", "sp"), None), P(),
        col_split, col_split, col_split, col_split, col_split, col_split,
        P("tp"), P("tp", None), P(("fs", "sp")), P(), P(),
        P("tp", None), P("tp", None),
    )
    return jax.shard_map(
        functools.partial(on_device, nz, ny),
        mesh=mesh,
        in_specs=placed,
        out_specs=(P(("fs", "sp"), None), P("tp", ("fs", "sp"))),
        check_vma=False,
    )
```
